1024 devices in a mesh: rep: 16 (over z), fs: 8 (over y), tp: 8 (over x, core).
Axes of the slice: x: 4, y: 8, z: 16, core: 2. Of those that a mesh axis runs over, the one named last changes fastest.
Arguments:
- tokens: bfloat16 [6144, 2048], P('rep', ('fs', 'tp')), may hold values from -6 to 6
- cotangent: bfloat16 [6144, 2048], P('rep', ('fs', 'tp')), may hold values from -16 to 16
- gain: float32 [2048], replicated, may hold values from 0.1 to 1.9
- w_gate: bfloat16 [5376, 2048], P(('fs', 'tp')), may hold values from -0.125 to 0.125
- w_up: bfloat16 [5376, 2048], P(('fs', 'tp')), may hold values from -0.125 to 0.125
- w_down: bfloat16 [5376, 2048], P(('fs', 'tp')), may hold values from -0.078125 to 0.078125
Outputs:
- grad_input: bfloat16 [6144, 2048], P('rep', ('fs', 'tp'))
- grad_gain: float32 [2048], P(('fs', 'tp'))
- grad_gate: float32 [5376, 2048], P(('fs', 'tp'))
- grad_up: float32 [5376, 2048], P(('fs', 'tp'))
- grad_down: float32 [5376, 2048], P(('fs', 'tp'))
The draws below stay inside these ranges and needn't reach their ends.
All inputs are finite; a program needn't handle non-finite values.
Results may differ from the reference program's by a relative error of at most 0.006.
Values may be sent and summed in bfloat16 or wider, within the bound.
No kernel may reach another device: no remote copies, remote signals or barrier semaphores. Data moves between devices by JAX's collectives and lax.ppermute only.
A program may use at most 64 MiB of HBM per device.

```python
import jax
import jax.numpy as jnp
from jax import lax

D = 2048
FF = 5376
TOKENS = 6144


def raised(array, key, source, target, parts, factor):
    def block_of(axis_at):
        return (jnp.arange(array.shape[axis_at]) // (array.shape[axis_at] // parts)).reshape((-1,) + (1,) * (array.ndim - 1 - axis_at))

    one_side = jax.random.permutation(key, parts)[block_of(target)]
    second = (block_of(target) + parts // 2) % parts
    return jnp.where((block_of(source) == one_side) | (block_of(source) == second), factor * array, array)


def block_scale(key, extent, pieces, least, top_value):
    loudness = 1.0
    for axis_at, parts in pieces:
        steps = jax.random.uniform(jax.random.fold_in(jax.random.fold_in(key, 6), axis_at), (parts,), jnp.float32, least / len(pieces), top_value / len(pieces))
        loudness = loudness * jnp.repeat(jnp.exp(steps), extent[axis_at] // parts).reshape((-1,) + (1,) * (len(extent) - 1 - axis_at))
    return loudness


def bell_draw(stream_key, dims, width, reach, pieces=(), held_as=jnp.bfloat16):
    level = block_scale(stream_key, dims, pieces, -0.22, 0.18) if pieces else 1.0
    values = jax.random.normal(stream_key, dims, jnp.float32) * width * level
    return jnp.minimum(jnp.maximum(values, -reach), reach).astype(held_as)


def noise_with(stream_key, dims, width, reach, pieces, heavy, kind=jnp.bfloat16):
    drawn = width * jax.random.normal(stream_key, dims, jnp.float32)
    if pieces:
        drawn = drawn * block_scale(stream_key, dims, pieces, -0.22, 0.18)
    return jnp.clip(raised(drawn, jax.random.fold_in(stream_key, 3), *heavy), -reach, reach).astype(kind)


def setup_inputs(seed: int = 0) -> dict:
    streams_of = jax.random.split(jax.random.key(seed), 7)
    tokens = bell_draw(streams_of[0], (TOKENS, D), 1.0, 6.0, ((0, 16), (1, 64)))
    cotangent = noise_with(streams_of[1], (TOKENS, D), 1.0, 16.0, ((0, 16), (1, 64)), (0, 1, 64, 4.0))
    gain = jnp.clip(1.0 + 0.18 * jax.random.normal(streams_of[2], (D,), jnp.float32), 0.1, 1.9)
    w_gate = bell_draw(streams_of[3], (FF, D), D ** -0.5, 0.125, ((0, 64),))
    w_up = bell_draw(streams_of[4], (FF, D), D ** -0.5, 0.125, ((0, 64),))
    w_down = bell_draw(streams_of[5], (FF, D), FF ** -0.5, 0.078125, ((0, 64),))
    return {"tokens": tokens, "cotangent": cotangent, "gain": gain, "w_gate": w_gate, "w_up": w_up, "w_down": w_down}


EPS = 1e-06

def reference(tokens, cotangent, gain, w_gate, w_up, w_down):
    xf = tokens.astype(jnp.float32)
    inv_rms = lax.rsqrt(lax.optimization_barrier(jnp.mean(xf * xf, axis=1, keepdims=True)) + EPS)
    unit = xf * inv_rms
    normed = (unit * gain).astype(jnp.bfloat16)
    gate = jnp.dot(normed, w_gate.T, preferred_element_type=jnp.float32)
    up = jnp.dot(normed, w_up.T, preferred_element_type=jnp.float32)
    sig = jax.nn.sigmoid(gate)
    active = gate * sig
    hidden = (active * up).astype(jnp.bfloat16)
    d_hidden = 0.5 * jnp.dot(cotangent, w_down.T, preferred_element_type=jnp.float32)
    d_gate = (d_hidden * up * sig * (1.0 + gate * (1.0 - sig))).astype(jnp.bfloat16)
    d_up = (d_hidden * active).astype(jnp.bfloat16)
    grad_down = 0.5 * jnp.dot(hidden.T, cotangent, preferred_element_type=jnp.float32)
    grad_gate = jnp.dot(d_gate.T, normed, preferred_element_type=jnp.float32)
    grad_up = jnp.dot(d_up.T, normed, preferred_element_type=jnp.float32)
    d_normed = jnp.dot(d_gate, w_gate, preferred_element_type=jnp.float32) + jnp.dot(d_up, w_up, preferred_element_type=jnp.float32)
    grad_gain = lax.optimization_barrier(jnp.sum(unit * d_normed, axis=0))
    d_unit = d_normed * gain
    row_mean = lax.optimization_barrier(jnp.mean(unit * d_unit, axis=1, keepdims=True))
    grad_input = (cotangent.astype(jnp.float32) + inv_rms * (d_unit - unit * row_mean)).astype(jnp.bfloat16)
    return (grad_input, grad_gain, grad_gate, grad_up, grad_down)
```

```python
import functools

import jax
import jax.numpy as jnp
from jax import lax
from jax.experimental import pallas as pl
from jax.experimental.pallas import tpu as pltpu
from jax.sharding import Mesh
from jax.sharding import PartitionSpec as P


FS_TP = ("fs", "tp_0", "tp_1")
EPS = 1e-06
BF = jnp.bfloat16
F32 = jnp.float32
LANES = 128
VMEM = pl.BlockSpec(memory_space=pltpu.VMEM)
ANY = pl.BlockSpec(memory_space=pl.ANY)


def sigmoid(v):
    return jax.nn.sigmoid(v)


def gain_columns(gain_ref, out_ref):
    for q in range(gain_ref.shape[0]):
        row = jnp.broadcast_to(gain_ref[q : q + 1, :], (LANES, LANES))
        out_ref[q * LANES : (q + 1) * LANES, :] = row.T


def main_kernel(
    sizes,
    own_ref,
    other_ref,
    gate_w_ref,
    up_w_ref,
    down_w_ref,
    gain_ref,
    part_ref,
    inv_ref,
    *rest,
):
    n_fs, n_x, n_core, tokens, hidden, padded, width, block = sizes
    n_pieces = 3 * (width // LANES)
    pieces = rest[:n_pieces]
    normed_s, cot_s, pair_s, down_s, delta_s, hidden_s, gain_s = rest[n_pieces:]
    core = lax.axis_index("tp_1")

    low = padded - 16
    pair_s[low:padded, :] = jnp.zeros((16, width), BF)
    pair_s[padded + low : 2 * padded, :] = jnp.zeros((16, width), BF)
    down_s[low:padded, :] = jnp.zeros((16, width), BF)
    pair_s[0:hidden, :] = gate_w_ref[...]
    pair_s[padded : padded + hidden, :] = up_w_ref[...]
    down_s[0:hidden, :] = down_w_ref[...]
    gain_columns(gain_ref, gain_s)

    def square_sum(s, acc):
        for ref in (own_ref, other_ref):
            v = ref[s, :, 0:tokens].astype(F32)
            v = v * v
            for k in range(block // 8):
                acc = acc + v[8 * k : 8 * k + 8, :]
        return acc

    total = lax.fori_loop(0, n_fs * n_x, square_sum, jnp.zeros((8, tokens), F32))
    mean = jnp.sum(total, axis=0, keepdims=True) / width
    inv = lax.rsqrt(mean + EPS)
    inv_ref[...] = jnp.broadcast_to(inv, (8, tokens))

    def normalise(s, carry):
        x = s // n_fs
        y = s % n_fs
        for ref, which in ((own_ref, core), (other_ref, 1 - core)):
            at = pl.multiple_of(((y * n_x + x) * n_core + which) * block, block)
            v = ref[s, :, 0:tokens].astype(F32) * inv
            g = gain_s[pl.ds(at, block), :]
            v = v * jnp.concatenate([g] * (tokens // LANES), axis=1)
            normed_s[pl.ds(at, block), :] = v.astype(BF)
            cot_s[pl.ds(at, block), :] = ref[s, :, tokens : 2 * tokens]
        return carry

    lax.fori_loop(0, n_fs * n_x, normalise, 0)

    both = jnp.dot(pair_s[...], normed_s[...], preferred_element_type=F32)
    d_hidden = 0.5 * jnp.dot(down_s[...], cot_s[...], preferred_element_type=F32)
    gate = both[0:padded, :]
    up = both[padded : 2 * padded, :]
    sig = sigmoid(gate)
    active = gate * sig
    hidden_s[...] = (active * up).astype(BF)
    d_gate = (d_hidden * up * sig * (1.0 + gate * (1.0 - sig))).astype(BF)
    d_up = (d_hidden * active).astype(BF)
    delta_s[0:padded, :] = d_gate
    delta_s[padded : 2 * padded, :] = d_up
    row = jnp.sum(d_gate.astype(F32) * gate + d_up.astype(F32) * up, axis=0, keepdims=True)
    high = row.astype(BF)
    rest_of = (row - high.astype(F32)).astype(BF)
    tail = jnp.concatenate(
        [high, rest_of, jnp.zeros((part_ref.shape[1] - block - 2, tokens), BF)], axis=0
    )
    for d in range(part_ref.shape[0]):
        part_ref[d, block:, :] = tail

    step = 256
    for b in range(width // step):
        cols = slice(b * step, (b + 1) * step)
        value = lax.dot_general(
            pair_s[:, cols], delta_s[...], (((0,), (0,)), ((), ())), preferred_element_type=F32
        ).astype(BF)
        for k in range(step // block):
            part_ref[b * (step // block) + k, 0:block, :] = value[k * block : (k + 1) * block, :]
    for b in range(width // step):
        rows = slice(b * step, (b + 1) * step)
        two = lax.dot_general(
            delta_s[...], normed_s[rows, :], (((1,), (1,)), ((), ())), preferred_element_type=F32
        )
        one = 0.5 * lax.dot_general(
            hidden_s[...], cot_s[rows, :], (((1,), (1,)), ((), ())), preferred_element_type=F32
        )
        for k in range(step // LANES):
            at = b * (step // LANES) + k
            lanes = slice(k * LANES, (k + 1) * LANES)
            pieces[at][...] = two[0:hidden, lanes]
            pieces[width // LANES + at][...] = two[padded : padded + hidden, lanes]
            pieces[2 * (width // LANES) + at][...] = one[0:hidden, lanes]


def weight_kernel(n_blocks, gate_w_ref, up_w_ref, gain_ref, one_ref, after_ref, *rest):
    pieces = rest[: 3 * n_blocks]
    gate_ref, up_ref, down_ref, slab_ref = rest[3 * n_blocks :]
    per = slab_ref.shape[0] // n_blocks
    for b in range(n_blocks):
        lanes = slice(b * LANES, (b + 1) * LANES)
        g, u = pieces[b][...], pieces[n_blocks + b][...]
        gate_ref[:, lanes] = g
        up_ref[:, lanes] = u
        down_ref[:, lanes] = pieces[2 * n_blocks + b][...]
        v = g * gate_w_ref[:, lanes].astype(F32) + u * up_w_ref[:, lanes].astype(F32)
        v = jnp.sum(v, axis=0, keepdims=True) / gain_ref[b : b + 1, :]
        v = jnp.broadcast_to(v, (8, LANES))
        for k in range(per):
            slab_ref[b * per + k] = v


def input_kernel(block, n_x, n_core, width, part_ref, tok_ref, cot_ref, inv_ref, gain_ref, out_ref, gain_s):
    sources, rows, tokens = part_ref.shape
    me = (lax.axis_index("fs") * n_x + lax.axis_index("tp_0")) * n_core + lax.axis_index("tp_1")
    gain_columns(gain_ref, gain_s)

    def add(s, acc):
        return acc + part_ref[s].astype(F32)

    total = lax.fori_loop(0, sources, add, jnp.zeros((rows, tokens), F32))
    summed = total[0:block, :]
    row = (total[block : block + 1, :] + total[block + 1 : block + 2, :]) / width
    inv = inv_ref[0:1, :]
    g = gain_s[pl.ds(pl.multiple_of(me * block, block), block), :]
    d_unit = summed * jnp.concatenate([g] * (tokens // LANES), axis=1)
    unit = tok_ref[...].astype(F32) * inv
    out_ref[...] = (cot_ref[...].astype(F32) + inv * (d_unit - unit * row)).astype(BF)


def spread(block, axis):
    n = lax.axis_size(axis)
    copies = jnp.broadcast_to(block[None], (n,) + block.shape)
    return lax.all_to_all(copies, axis, 0, 0, tiled=True)


def body(tokens, cotangent, gain, w_gate, w_up, w_down):
    n_fs, n_x, n_core = (lax.axis_size(a) for a in FS_TP)
    members = n_fs * n_x * n_core
    rows, block = tokens.shape
    width = gain.shape[0]
    hidden = w_gate.shape[0]
    padded = -(-hidden // 32) * 32
    n_blocks = width // LANES
    tok_t, cot_t = tokens.T, cotangent.T
    both = jnp.concatenate([tok_t, cot_t], axis=1)
    column = spread(both, "fs")
    plane = spread(column.reshape(n_fs * block, 2 * rows), "tp_0")
    plane = plane.reshape(n_fs * n_x, block, 2 * rows)
    other = lax.ppermute(plane, "tp_1", [(0, 1), (1, 0)])
    gain_rows = gain.reshape(n_blocks, LANES)

    sizes = (n_fs, n_x, n_core, rows, hidden, padded, width, block)
    outs = pl.pallas_call(
        functools.partial(main_kernel, sizes),
        out_shape=[
            jax.ShapeDtypeStruct((members, block + 8, rows), BF),
            jax.ShapeDtypeStruct((8, rows), F32),
        ]
        + [jax.ShapeDtypeStruct((hidden, LANES), F32)] * (3 * n_blocks),
        in_specs=[VMEM] * 6,
        out_specs=[VMEM] * (2 + 3 * n_blocks),
        scratch_shapes=[
            pltpu.VMEM((width, rows), BF),
            pltpu.VMEM((width, rows), BF),
            pltpu.VMEM((2 * padded, width), BF),
            pltpu.VMEM((padded, width), BF),
            pltpu.VMEM((2 * padded, rows), BF),
            pltpu.VMEM((padded, rows), BF),
            pltpu.VMEM((width, LANES), F32),
        ],
        compiler_params=pltpu.CompilerParams(vmem_limit_bytes=30 * 2**20),
        cost_estimate=pl.CostEstimate(flops=11 * 10**8, bytes_accessed=10**7, transcendentals=0),
        name="main",
    )(plane, other, w_gate, w_up, w_down, gain_rows)
    part, inv, pieces = outs[0], outs[1], outs[2:]

    parts = lax.all_to_all(part, FS_TP, 0, 0, tiled=True)
    one = inv[0:1, 0:1]
    *pieces, one = lax.psum((*pieces, one), "rep")

    grad_gate, grad_up, grad_down, slabs = pl.pallas_call(
        functools.partial(weight_kernel, n_blocks),
        out_shape=[jax.ShapeDtypeStruct((hidden, width), F32)] * 3
        + [jax.ShapeDtypeStruct((members, 8, LANES), F32)],
        in_specs=[VMEM] * 4 + [ANY] + [VMEM] * (3 * n_blocks),
        out_specs=[VMEM] * 4,
        compiler_params=pltpu.CompilerParams(vmem_limit_bytes=20 * 2**20),
        name="weights",
    )(w_gate, w_up, gain_rows, one, parts, *pieces)

    slabs = lax.all_to_all(slabs, FS_TP, 0, 0, tiled=True)
    grad_input = pl.pallas_call(
        functools.partial(input_kernel, block, n_x, n_core, width),
        out_shape=jax.ShapeDtypeStruct((block, rows), BF),
        in_specs=[VMEM] * 5,
        out_specs=VMEM,
        scratch_shapes=[pltpu.VMEM((width, LANES), F32)],
        compiler_params=pltpu.CompilerParams(vmem_limit_bytes=20 * 2**20),
        cost_estimate=pl.CostEstimate(flops=10**8, bytes_accessed=2 * 10**6, transcendentals=0),
        name="input",
    )(parts, tok_t, cot_t, inv, gain_rows)
    me = lax.axis_index(FS_TP) % (LANES // block)
    grad_gain = lax.dynamic_slice_in_dim(jnp.sum(slabs[:, 0, :], axis=0), me * block, block, 0)
    return (grad_input.T, grad_gain, grad_gate, grad_up, grad_down)


def solution(mesh):
    torus = Mesh(
        mesh.devices.reshape(mesh.shape["rep"], mesh.shape["fs"], 4, 2),
        ("rep", "fs", "tp_0", "tp_1"),
    )
    placed = (P("rep", FS_TP), P("rep", FS_TP), P(), P(FS_TP, None), P(FS_TP, None), P(FS_TP, None))
    return jax.shard_map(
        body,
        mesh=torus,
        in_specs=placed,
        out_specs=(P("rep", FS_TP), P(FS_TP), P(FS_TP, None), P(FS_TP, None), P(FS_TP, None)),
        check_vma=False,
    )
```

```python
import functools

import jax
import jax.numpy as jnp
from jax import lax
from jax.experimental import pallas as pl
from jax.experimental.pallas import tpu as pltpu
from jax.sharding import Mesh
from jax.sharding import PartitionSpec as P


FS_TP = ("fs", "tp_0", "tp_1")
EPS = 1e-06
BF = jnp.bfloat16
F32 = jnp.float32
LANES = 128
VMEM = pl.BlockSpec(memory_space=pltpu.VMEM)


def gain_columns(gain_ref, out_ref):
    for q in range(gain_ref.shape[0]):
        row = jnp.broadcast_to(gain_ref[q : q + 1, :], (LANES, LANES))
        out_ref[q * LANES : (q + 1) * LANES, :] = row.T


def split_in_two(v):
    high = v.astype(BF)
    return high, (v - high.astype(F32)).astype(BF)


def main_kernel(
    sizes,
    own_ref,
    other_ref,
    gate_w_ref,
    up_w_ref,
    down_w_ref,
    gain_ref,
    keep_ref,
    send_ref,
    row_ref,
    inv_ref,
    far_ref,
    near_ref,
    back_ref,
    stay_ref,
    normed_s,
    cot_s,
    pair_s,
    down_s,
    delta_s,
    hidden_s,
    gain_s,
    part_s,
    grad_s,
):
    n_rep, n_fs, n_x, n_core, tokens, hidden, padded, width, block = sizes
    core = lax.axis_index("tp_1")
    z = lax.axis_index("rep")
    tall = grad_s.shape[1]

    low = padded - 16
    pair_s[low:padded, :] = jnp.zeros((16, width), BF)
    pair_s[padded + low : 2 * padded, :] = jnp.zeros((16, width), BF)
    down_s[low:padded, :] = jnp.zeros((16, width), BF)
    pair_s[0:hidden, :] = gate_w_ref[...]
    pair_s[padded : padded + hidden, :] = up_w_ref[...]
    down_s[0:hidden, :] = down_w_ref[...]
    gain_columns(gain_ref, gain_s)

    def square_sum(s, acc):
        for ref in (own_ref, other_ref):
            v = ref[s, :, 0:tokens].astype(F32)
            v = v * v
            for k in range(block // 8):
                acc = acc + v[8 * k : 8 * k + 8, :]
        return acc

    total = lax.fori_loop(0, n_fs * n_x, square_sum, jnp.zeros((8, tokens), F32))
    mean = jnp.sum(total, axis=0, keepdims=True) / width
    inv = lax.rsqrt(mean + EPS)
    inv_ref[...] = jnp.broadcast_to(inv, (8, tokens))

    def normalise(s, carry):
        x = s // n_fs
        y = s % n_fs
        for ref, which in ((own_ref, core), (other_ref, 1 - core)):
            at = pl.multiple_of(((y * n_x + x) * n_core + which) * block, block)
            v = ref[s, :, 0:tokens].astype(F32) * inv
            g = gain_s[pl.ds(at, block), :]
            v = v * jnp.concatenate([g] * (tokens // LANES), axis=1)
            normed_s[pl.ds(at, block), :] = v.astype(BF)
            cot_s[pl.ds(at, block), :] = ref[s, :, tokens : 2 * tokens]
        return carry

    lax.fori_loop(0, n_fs * n_x, normalise, 0)

    both = jnp.dot(pair_s[...], normed_s[...], preferred_element_type=F32)
    d_hidden = 0.5 * jnp.dot(down_s[...], cot_s[...], preferred_element_type=F32)
    gate = both[0:padded, :]
    up = both[padded : 2 * padded, :]
    sig = jax.nn.sigmoid(gate)
    active = gate * sig
    hidden_s[...] = (active * up).astype(BF)
    d_gate = (d_hidden * up * sig * (1.0 + gate * (1.0 - sig))).astype(BF)
    d_up = (d_hidden * active).astype(BF)
    delta_s[0:padded, :] = d_gate
    delta_s[padded : 2 * padded, :] = d_up
    row = jnp.sum(d_gate.astype(F32) * gate + d_up.astype(F32) * up, axis=0, keepdims=True)
    row_ref[...] = jnp.broadcast_to(row, (8, tokens))
    high, low_part = split_in_two(row)
    send_ref[n_fs * n_x] = jnp.concatenate(
        [high, low_part, jnp.zeros((block - 2, tokens), BF)], axis=0
    )

    step = 256
    for b in range(width // step):
        cols = slice(b * step, (b + 1) * step)
        value = lax.dot_general(
            pair_s[:, cols], delta_s[...], (((0,), (0,)), ((), ())), preferred_element_type=F32
        ).astype(BF)
        for k in range(step // block):
            part_s[b * (step // block) + k] = value[k * block : (k + 1) * block, :]

    def share(s, carry):
        keep_ref[s] = part_s[n_core * s + core]
        send_ref[s] = part_s[n_core * s + 1 - core]
        return carry

    lax.fori_loop(0, n_fs * n_x, share, 0)

    for b in range(width // step):
        rows = slice(b * step, (b + 1) * step)
        two = lax.dot_general(
            delta_s[...], normed_s[rows, :], (((1,), (1,)), ((), ())), preferred_element_type=F32
        )
        one = 0.5 * lax.dot_general(
            hidden_s[...], cot_s[rows, :], (((1,), (1,)), ((), ())), preferred_element_type=F32
        )
        for k in range(step // LANES):
            at = b * (step // LANES) + k
            lanes = slice(k * LANES, (k + 1) * LANES)
            grad_s[at, :, 0:LANES] = two[0:tall, lanes]
            grad_s[at, :, LANES : 2 * LANES] = two[padded : padded + tall, lanes]
            grad_s[at, :, 2 * LANES : 3 * LANES] = one[0:tall, lanes]

    side = 1 - 2 * core
    for i in range(4):
        for ref, base in ((far_ref, 4), (near_ref, 3), (back_ref, 1), (stay_ref, 2)):
            chunk = lax.rem(z + side * (base + 4 * i) + 2 * n_rep, n_rep)
            ref[i] = grad_s[chunk].astype(ref.dtype)


def core_kernel(block, keep_ref, got_ref, row_ref, out_ref):
    slabs = keep_ref.shape[0]
    tokens = keep_ref.shape[2]
    other = got_ref[slabs, 0:8, :].astype(F32)
    row = row_ref[0:1, :] + other[0:1, :] + other[1:2, :]
    high, low_part = split_in_two(row)
    tail = jnp.concatenate([high, low_part, jnp.zeros((6, tokens), BF)], axis=0)

    def add(s, carry):
        v = keep_ref[s].astype(F32) + got_ref[s].astype(F32)
        out_ref[s, 0:block, :] = v.astype(BF)
        out_ref[s, block : block + 8, :] = tail
        return carry

    lax.fori_loop(0, slabs, add, 0)


def stop_kernel(far_ref, near_ref, back_ref, stay_ref, *out_refs):
    for i, out_ref in enumerate(out_refs):
        v = stay_ref[i] + far_ref[i].astype(F32) + near_ref[i].astype(F32) + back_ref[i].astype(F32)
        out_ref[...] = v.astype(BF)


def owner_kernel(
    sizes,
    part_ref,
    tok_ref,
    cot_ref,
    inv_ref,
    gain_ref,
    a_ref,
    b_ref,
    c_ref,
    d_ref,
    input_ref,
    chunk_ref,
    gain_s,
):
    n_x, n_core, width, hidden, block = sizes
    sources, rows, tokens = part_ref.shape
    me = (lax.axis_index("fs") * n_x + lax.axis_index("tp_0")) * n_core + lax.axis_index("tp_1")
    gain_columns(gain_ref, gain_s)

    def add(s, acc):
        return acc + part_ref[s].astype(F32)

    total = lax.fori_loop(0, sources, add, jnp.zeros((rows, tokens), F32))
    summed = total[0:block, :]
    row = (total[block : block + 1, :] + total[block + 1 : block + 2, :]) / width
    inv = inv_ref[0:1, :]
    g = gain_s[pl.ds(pl.multiple_of(me * block, block), block), :]
    d_unit = summed * jnp.concatenate([g] * (tokens // LANES), axis=1)
    unit = tok_ref[...].astype(F32) * inv
    input_ref[...] = (cot_ref[...].astype(F32) + inv * (d_unit - unit * row)).astype(BF)

    along = jnp.sum(unit * summed, axis=1, keepdims=True)
    square = jnp.concatenate(
        [jnp.broadcast_to(along, (block, LANES)), jnp.zeros((LANES - block, LANES), F32)], axis=0
    )
    v = square.T[0:8, :]
    high, mid = split_in_two(v)
    low = v - high.astype(F32) - mid.astype(F32)
    extra = jnp.concatenate([high.astype(F32), mid.astype(F32), low], axis=1)[0:1, :]
    chunk = a_ref[...].astype(F32) + b_ref[...].astype(F32) + c_ref[...].astype(F32) + d_ref[...].astype(F32)
    which = lax.broadcasted_iota(jnp.int32, chunk.shape, 0)
    chunk = jnp.where(which == hidden, jnp.broadcast_to(extra, chunk.shape), chunk)
    chunk_ref[...] = chunk[0 : hidden + 1, :].astype(BF)


def out_kernel(all_ref, gate_ref, up_ref, down_ref, gain_ref):
    n, tall, _ = all_ref.shape
    hidden = tall - 1
    total = jnp.zeros((1, 3 * LANES), F32)
    for b in range(n):
        lanes = slice(b * LANES, (b + 1) * LANES)
        v = all_ref[b].astype(F32)
        gate_ref[:, lanes] = v[0:hidden, 0:LANES]
        up_ref[:, lanes] = v[0:hidden, LANES : 2 * LANES]
        down_ref[:, lanes] = v[0:hidden, 2 * LANES : 3 * LANES]
        total = total + v[hidden : hidden + 1, :]
    gain = total[:, 0:LANES] + total[:, LANES : 2 * LANES] + total[:, 2 * LANES : 3 * LANES]
    gain_ref[...] = gain[:, 0 : gain_ref.shape[1]]


def spread(block, axis):
    n = lax.axis_size(axis)
    copies = jnp.broadcast_to(block[None], (n,) + block.shape)
    return lax.all_to_all(copies, axis, 0, 0, tiled=True)


def shifted(v, by):
    n = lax.axis_size("rep")
    pairs = []
    for z in range(n):
        pairs.append((z * 2, (z + by) % n * 2))
        pairs.append((z * 2 + 1, (z - by) % n * 2 + 1))
    return lax.ppermute(v, ("rep", "tp_1"), pairs)


def body(tokens, cotangent, gain, w_gate, w_up, w_down):
    n_rep = lax.axis_size("rep")
    n_fs, n_x, n_core = (lax.axis_size(a) for a in FS_TP)
    peers = n_fs * n_x
    rows, block = tokens.shape
    width = gain.shape[0]
    hidden = w_gate.shape[0]
    padded = -(-hidden // 32) * 32
    tall = -(-hidden // 8) * 8
    n_blocks = width // LANES
    tok_t, cot_t = tokens.T, cotangent.T
    both = jnp.concatenate([tok_t, cot_t], axis=1)
    column = spread(both, "fs")
    plane = spread(column.reshape(n_fs * block, 2 * rows), "tp_0")
    plane = plane.reshape(peers, block, 2 * rows)
    other = lax.ppermute(plane, "tp_1", [(0, 1), (1, 0)])
    gain_rows = gain.reshape(n_blocks, LANES)

    def shape(*dims, dtype=BF):
        return jax.ShapeDtypeStruct(dims, dtype)

    sizes = (n_rep, n_fs, n_x, n_core, rows, hidden, padded, width, block)
    group = (4, tall, 3 * LANES)
    keep, send, row, inv, far, near, back, stay = pl.pallas_call(
        functools.partial(main_kernel, sizes),
        out_shape=[
            shape(peers, block, rows),
            shape(peers + 1, block, rows),
            shape(8, rows, dtype=F32),
            shape(8, rows, dtype=F32),
            shape(*group),
            shape(*group),
            shape(*group),
            shape(*group, dtype=F32),
        ],
        in_specs=[VMEM] * 6,
        out_specs=[VMEM] * 8,
        scratch_shapes=[
            pltpu.VMEM((width, rows), BF),
            pltpu.VMEM((width, rows), BF),
            pltpu.VMEM((2 * padded, width), BF),
            pltpu.VMEM((padded, width), BF),
            pltpu.VMEM((2 * padded, rows), BF),
            pltpu.VMEM((padded, rows), BF),
            pltpu.VMEM((width, LANES), F32),
            pltpu.VMEM((peers * n_core, block, rows), BF),
            pltpu.VMEM((n_blocks, tall, 3 * LANES), F32),
        ],
        compiler_params=pltpu.CompilerParams(vmem_limit_bytes=34 * 2**20),
        cost_estimate=pl.CostEstimate(flops=11 * 10**8, bytes_accessed=10**7, transcendentals=0),
        name="main",
    )(plane, other, w_gate, w_up, w_down, gain_rows)

    got = lax.ppermute(send, "tp_1", [(0, 1), (1, 0)])
    far = shifted(far, 2)
    near = shifted(near, 1)
    back = shifted(back, -1)
    ready = pl.pallas_call(
        functools.partial(core_kernel, block),
        out_shape=shape(peers, block + 8, rows),
        in_specs=[VMEM] * 3,
        out_specs=VMEM,
        compiler_params=pltpu.CompilerParams(vmem_limit_bytes=8 * 2**20),
        cost_estimate=pl.CostEstimate(flops=10**6, bytes_accessed=3 * 10**6, transcendentals=0),
        name="core",
    )(keep, got, row)
    parts = lax.all_to_all(ready, FS_TP[:2], 0, 0, tiled=True)
    sums = pl.pallas_call(
        stop_kernel,
        out_shape=[shape(tall, 3 * LANES)] * 4,
        in_specs=[VMEM] * 4,
        out_specs=[VMEM] * 4,
        compiler_params=pltpu.CompilerParams(vmem_limit_bytes=8 * 2**20),
        cost_estimate=pl.CostEstimate(flops=10**6, bytes_accessed=2 * 10**6, transcendentals=0),
        name="stop",
    )(far, near, back, stay)
    sums = [shifted(s, by) for s, by in zip(sums, (2, 6, -6, -2))]

    grad_input, chunk = pl.pallas_call(
        functools.partial(owner_kernel, (n_x, n_core, width, hidden, block)),
        out_shape=[shape(block, rows), shape(hidden + 1, 3 * LANES)],
        in_specs=[VMEM] * 9,
        out_specs=[VMEM] * 2,
        scratch_shapes=[pltpu.VMEM((width, LANES), F32)],
        compiler_params=pltpu.CompilerParams(vmem_limit_bytes=12 * 2**20),
        cost_estimate=pl.CostEstimate(flops=10**8, bytes_accessed=2 * 10**6, transcendentals=0),
        name="owner",
    )(parts, tok_t, cot_t, inv, gain_rows, *sums)
    everything = lax.all_gather(chunk, "rep", axis=0, tiled=False)
    grad_gate, grad_up, grad_down, grad_gain = pl.pallas_call(
        out_kernel,
        out_shape=[shape(hidden, width, dtype=F32)] * 3 + [shape(1, block, dtype=F32)],
        in_specs=[VMEM],
        out_specs=[VMEM] * 4,
        compiler_params=pltpu.CompilerParams(vmem_limit_bytes=12 * 2**20),
        name="out",
    )(everything)
    return (grad_input.T, grad_gain.reshape(block), grad_gate, grad_up, grad_down)


def solution(mesh):
    torus = Mesh(
        mesh.devices.reshape(mesh.shape["rep"], mesh.shape["fs"], 4, 2),
        ("rep", "fs", "tp_0", "tp_1"),
    )
    placed = (P("rep", FS_TP), P("rep", FS_TP), P(), P(FS_TP, None), P(FS_TP, None), P(FS_TP, None))
    return jax.shard_map(
        body,
        mesh=torus,
        in_specs=placed,
        out_specs=(P("rep", FS_TP), P(FS_TP), P(FS_TP, None), P(FS_TP, None), P(FS_TP, None)),
        check_vma=False,
    )
```

```python
import functools

import jax
import jax.numpy as jnp
from jax import lax
from jax.experimental import pallas as pl
from jax.experimental.pallas import tpu as pltpu
from jax.sharding import Mesh
from jax.sharding import PartitionSpec as P


FS_TP = ("fs", "tp_0", "tp_1")
EPS = 1e-06
BF = jnp.bfloat16
F32 = jnp.float32
LANES = 128
VMEM = pl.BlockSpec(memory_space=pltpu.VMEM)
ANY = pl.BlockSpec(memory_space=pl.ANY)


def gain_columns(gain_ref, out_ref):
    for q in range(gain_ref.shape[0]):
        row = jnp.broadcast_to(gain_ref[q : q + 1, :], (LANES, LANES))
        out_ref[q * LANES : (q + 1) * LANES, :] = row.T


def split_in_two(v):
    high = v.astype(BF)
    return high, (v - high.astype(F32)).astype(BF)


def square_sum(ref, tokens):
    slabs, block, _ = ref.shape

    def step(s, acc):
        v = ref[s, :, 0:tokens].astype(F32)
        v = v * v
        parts = [v[8 * k : 8 * k + 8, :] for k in range(block // 8)]
        while len(parts) > 1:
            parts = [a + b for a, b in zip(parts[::2], parts[1::2])]
        return acc + parts[0]

    return lax.fori_loop(0, slabs, step, jnp.zeros((8, tokens), F32), unroll=4)


def ready_kernel(
    tokens, own_ref, gate_w_ref, up_w_ref, down_w_ref, gain_ref, pair_ref, down_ref, columns_ref, square_ref
):
    hidden, width = gate_w_ref.shape
    padded = down_ref.shape[0]
    low = padded - 16
    pair_ref[low:padded, :] = jnp.zeros((16, width), BF)
    pair_ref[padded + low : 2 * padded, :] = jnp.zeros((16, width), BF)
    down_ref[low:padded, :] = jnp.zeros((16, width), BF)
    pair_ref[0:hidden, :] = gate_w_ref[...]
    pair_ref[padded : padded + hidden, :] = up_w_ref[...]
    down_ref[0:hidden, :] = down_w_ref[...]
    gain_columns(gain_ref, columns_ref)
    square_ref[...] = square_sum(own_ref, tokens)


def main_kernel(
    sizes,
    own_ref,
    other_ref,
    pair_s,
    down_s,
    gain_s,
    square_ref,
    keep_ref,
    send_ref,
    row_ref,
    inv_ref,
    far_ref,
    near_ref,
    back_ref,
    stay_ref,
    normed_s,
    cot_s,
    delta_s,
    hidden_s,
    part_s,
    grad_s,
):
    n_rep, n_fs, n_x, n_core, tokens, _, padded, width, block = sizes
    core = lax.axis_index("tp_1")
    z = lax.axis_index("rep")
    tall = grad_s.shape[1]
    total = square_ref[...] + square_sum(other_ref, tokens)
    mean = jnp.sum(total, axis=0, keepdims=True) / width
    inv = lax.rsqrt(mean + EPS)
    inv_ref[...] = jnp.broadcast_to(inv, (8, tokens))

    def normalise(s, carry):
        x = n_x - 1 - s // n_fs
        y = n_fs - 1 - s % n_fs
        for ref, which in ((own_ref, core), (other_ref, 1 - core)):
            at = pl.multiple_of(((y * n_x + x) * n_core + which) * block, block)
            v = ref[s, :, 0:tokens].astype(F32) * inv
            g = gain_s[pl.ds(at, block), :]
            v = v * jnp.concatenate([g] * (tokens // LANES), axis=1)
            normed_s[pl.ds(at, block), :] = v.astype(BF)
            cot_s[pl.ds(at, block), :] = ref[s, :, tokens : 2 * tokens]
        return carry

    lax.fori_loop(0, n_fs * n_x, normalise, 0)

    both = jnp.dot(pair_s[...], normed_s[...], preferred_element_type=F32)
    d_hidden = 0.5 * jnp.dot(down_s[...], cot_s[...], preferred_element_type=F32)
    gate = both[0:padded, :]
    up = both[padded : 2 * padded, :]
    sig = jax.nn.sigmoid(gate)
    active = gate * sig
    hidden_s[...] = (active * up).astype(BF)
    d_gate = (d_hidden * up * sig * (1.0 + gate * (1.0 - sig))).astype(BF)
    d_up = (d_hidden * active).astype(BF)
    delta_s[0:padded, :] = d_gate
    delta_s[padded : 2 * padded, :] = d_up
    row = jnp.sum(d_gate.astype(F32) * gate + d_up.astype(F32) * up, axis=0, keepdims=True)
    row_ref[...] = jnp.broadcast_to(row, (8, tokens))
    high, low_part = split_in_two(row)
    send_ref[n_fs * n_x] = jnp.concatenate(
        [high, low_part, jnp.zeros((block - 2, tokens), BF)], axis=0
    )

    step = 256
    for b in range(width // step):
        cols = slice(b * step, (b + 1) * step)
        value = lax.dot_general(
            pair_s[:, cols], delta_s[...], (((0,), (0,)), ((), ())), preferred_element_type=F32
        ).astype(BF)
        for k in range(step // block):
            part_s[b * (step // block) + k] = value[k * block : (k + 1) * block, :]

    def share(s, carry):
        keep_ref[s] = part_s[n_core * s + core]
        send_ref[s] = part_s[n_core * s + 1 - core]
        return carry

    lax.fori_loop(0, n_fs * n_x, share, 0, unroll=4)

    side = 1 - 2 * core
    for b in range(width // step):
        rows = slice(b * step, (b + 1) * step)
        two = lax.dot_general(
            delta_s[...], normed_s[rows, :], (((1,), (1,)), ((), ())), preferred_element_type=F32
        )
        one = 0.5 * lax.dot_general(
            hidden_s[...], cot_s[rows, :], (((1,), (1,)), ((), ())), preferred_element_type=F32
        )
        for k in range(step // LANES):
            at = b * (step // LANES) + k
            lanes = slice(k * LANES, (k + 1) * LANES)
            grad_s[at, :, 0:LANES] = two[0:tall, lanes].astype(BF)
            grad_s[at, :, LANES : 2 * LANES] = two[padded : padded + tall, lanes].astype(BF)
            grad_s[at, :, 2 * LANES : 3 * LANES] = one[0:tall, lanes].astype(BF)

    for i in range(4):
        for ref, base in ((far_ref, 4), (near_ref, 3), (back_ref, 1), (stay_ref, 2)):
            ref[i] = grad_s[lax.rem(z + side * (base + 4 * i) + 2 * n_rep, n_rep)]


def core_kernel(block, keep_ref, got_ref, row_ref, out_ref, slab_s, sems):
    slabs = got_ref.shape[0] - 1
    groups = got_ref.shape[2] // LANES
    pieces = sems.shape[0]
    each = slabs // pieces
    other = got_ref[slabs, 0:8, :].astype(F32)
    row = row_ref[0:1, :] + other[0:1, :] + other[1:2, :]
    high, low_part = split_in_two(row)
    tail = [v[:, k * LANES : (k + 1) * LANES] for v in (high, low_part) for k in range(groups)]
    tail = jnp.concatenate(tail + [jnp.zeros((8 - 2 * groups, LANES), BF)], axis=0)

    def add(s, carry):
        v = (keep_ref[s].astype(F32) + got_ref[s].astype(F32)).astype(BF)
        for k in range(groups):
            slab_s[s, k * block : (k + 1) * block, :] = v[:, k * LANES : (k + 1) * LANES]
        slab_s[s, groups * block : groups * block + 8, :] = tail
        return carry

    copies = []
    for p in range(pieces):
        lax.fori_loop(p * each, (p + 1) * each, add, 0, unroll=4)
        here = pl.ds(p * each, each)
        copies.append(pltpu.make_async_copy(slab_s.at[here], out_ref.at[here], sems.at[p]))
        copies[-1].start()
    for copy in copies:
        copy.wait()


def stop_kernel(far_ref, near_ref, back_ref, stay_ref, *out_refs):
    for i, out_ref in enumerate(out_refs):
        v = stay_ref[i].astype(F32) + far_ref[i].astype(F32)
        v = v + near_ref[i].astype(F32) + back_ref[i].astype(F32)
        out_ref[...] = v.astype(BF)


def owner_kernel(
    sizes,
    part_ref,
    tok_ref,
    cot_ref,
    inv_ref,
    gain_ref,
    a_ref,
    b_ref,
    c_ref,
    d_ref,
    input_ref,
    chunk_ref,
    column_s,
):
    n_x, n_core, width, hidden, block = sizes
    sources, rows, _ = part_ref.shape
    tokens = tok_ref.shape[1]
    groups = tokens // LANES

    def add(s, acc):
        return acc + part_ref[s].astype(F32)

    total = lax.fori_loop(0, sources, add, jnp.zeros((rows, LANES), F32), unroll=4)
    summed = jnp.concatenate([total[k * block : (k + 1) * block, :] for k in range(groups)], axis=1)
    at = groups * block
    row = [total[at + k : at + k + 1, :] + total[at + groups + k : at + groups + k + 1, :] for k in range(groups)]
    row = jnp.concatenate(row, axis=1) / width
    me = (lax.axis_index("fs") * n_x + lax.axis_index("tp_0")) * n_core + lax.axis_index("tp_1")
    per = LANES // block
    mine = gain_ref[pl.ds(lax.div(me, per), 1), :]
    column_s[...] = jnp.broadcast_to(mine, (LANES, LANES)).T
    g = column_s[pl.ds(pl.multiple_of(lax.rem(me, per) * block, block), block), :]
    inv = inv_ref[0:1, :]
    d_unit = summed * jnp.concatenate([g] * groups, axis=1)
    unit = tok_ref[...].astype(F32) * inv
    input_ref[...] = (cot_ref[...].astype(F32) + inv * (d_unit - unit * row)).astype(BF)

    along = jnp.sum(unit * summed, axis=1, keepdims=True)
    square = jnp.concatenate(
        [jnp.broadcast_to(along, (block, LANES)), jnp.zeros((LANES - block, LANES), F32)], axis=0
    )
    v = square.T[0:8, :]
    high, mid = split_in_two(v)
    low = v - high.astype(F32) - mid.astype(F32)
    extra = jnp.concatenate([high.astype(F32), mid.astype(F32), low], axis=1)[0:1, :]
    chunk = a_ref[...].astype(F32) + b_ref[...].astype(F32) + c_ref[...].astype(F32) + d_ref[...].astype(F32)
    which = lax.broadcasted_iota(jnp.int32, chunk.shape, 0)
    chunk = jnp.where(which == hidden, jnp.broadcast_to(extra, chunk.shape), chunk)
    chunk_ref[...] = chunk[0 : hidden + 1, :].astype(BF)


def out_kernel(all_ref, made_ref, gate_ref, up_ref, down_ref, gain_ref, input_ref):
    n, tall, _ = all_ref.shape
    hidden = tall - 1
    input_ref[...] = made_ref[...]
    total = jnp.zeros((1, 3 * LANES), F32)
    for b in range(n):
        lanes = slice(b * LANES, (b + 1) * LANES)
        v = all_ref[b].astype(F32)
        gate_ref[:, lanes] = v[0:hidden, 0:LANES]
        up_ref[:, lanes] = v[0:hidden, LANES : 2 * LANES]
        down_ref[:, lanes] = v[0:hidden, 2 * LANES : 3 * LANES]
        total = total + v[hidden : hidden + 1, :]
    gain = total[:, 0:LANES] + total[:, LANES : 2 * LANES] + total[:, 2 * LANES : 3 * LANES]
    gain_ref[...] = gain[:, 0 : gain_ref.shape[1]]


def spread(block, axis):
    n = lax.axis_size(axis)
    copies = jnp.broadcast_to(block[None], (n,) + block.shape)
    backwards = [list(range(n - 1, -1, -1))]
    return lax.all_to_all(copies, axis, 0, 0, tiled=True, axis_index_groups=backwards)


def shifted(v, by):
    n = lax.axis_size("rep")
    pairs = []
    for z in range(n):
        pairs.append((z * 2, (z + by) % n * 2))
        pairs.append((z * 2 + 1, (z - by) % n * 2 + 1))
    return lax.ppermute(v, ("rep", "tp_1"), pairs)


def body(tokens, cotangent, gain, w_gate, w_up, w_down):
    n_rep = lax.axis_size("rep")
    n_fs, n_x, n_core = (lax.axis_size(a) for a in FS_TP)
    peers = n_fs * n_x
    rows, block = tokens.shape
    width = gain.shape[0]
    hidden = w_gate.shape[0]
    padded = -(-hidden // 32) * 32
    tall = -(-hidden // 8) * 8
    n_blocks = width // LANES
    tok_t, cot_t = tokens.T, cotangent.T
    both = jnp.concatenate([tok_t, cot_t], axis=1)
    column = spread(both, "fs")
    plane = spread(column.reshape(n_fs * block, 2 * rows), "tp_0")
    plane = plane.reshape(peers, block, 2 * rows)
    other = lax.ppermute(plane, "tp_1", [(0, 1), (1, 0)])
    gain_rows = gain.reshape(n_blocks, LANES)

    def shape(*dims, dtype=BF):
        return jax.ShapeDtypeStruct(dims, dtype)

    pair, down, columns, square = pl.pallas_call(
        functools.partial(ready_kernel, rows),
        out_shape=[
            shape(2 * padded, width),
            shape(padded, width),
            shape(width, LANES, dtype=F32),
            shape(8, rows, dtype=F32),
        ],
        in_specs=[VMEM] * 5,
        out_specs=[VMEM] * 4,
        compiler_params=pltpu.CompilerParams(vmem_limit_bytes=8 * 2**20),
        cost_estimate=pl.CostEstimate(flops=10**7, bytes_accessed=4 * 10**6, transcendentals=0),
        name="ready",
    )(plane, w_gate, w_up, w_down, gain_rows)

    sizes = (n_rep, n_fs, n_x, n_core, rows, hidden, padded, width, block)
    group = (4, tall, 3 * LANES)
    keep, send, row, inv, far, near, back, stay = pl.pallas_call(
        functools.partial(main_kernel, sizes),
        out_shape=[
            shape(peers, block, rows),
            shape(peers + 1, block, rows),
            shape(8, rows, dtype=F32),
            shape(8, rows, dtype=F32),
            shape(*group),
            shape(*group),
            shape(*group),
            shape(*group),
        ],
        in_specs=[VMEM] * 6,
        out_specs=[VMEM] * 8,
        scratch_shapes=[
            pltpu.VMEM((width, rows), BF),
            pltpu.VMEM((width, rows), BF),
            pltpu.VMEM((2 * padded, rows), BF),
            pltpu.VMEM((padded, rows), BF),
            pltpu.VMEM((peers * n_core, block, rows), BF),
            pltpu.VMEM((n_blocks, tall, 3 * LANES), BF),
        ],
        compiler_params=pltpu.CompilerParams(vmem_limit_bytes=34 * 2**20),
        cost_estimate=pl.CostEstimate(flops=11 * 10**8, bytes_accessed=10**7, transcendentals=0),
        name="main",
    )(plane, other, pair, down, columns, square)

    got = lax.ppermute(send, "tp_1", [(0, 1), (1, 0)])
    far = shifted(far, 2)
    near = shifted(near, 1)
    back = shifted(back, -1)
    ready = pl.pallas_call(
        functools.partial(core_kernel, block),
        out_shape=shape(peers, block * (rows // LANES) + 8, LANES),
        in_specs=[VMEM] * 3,
        out_specs=ANY,
        scratch_shapes=[
            pltpu.VMEM((peers, block * (rows // LANES) + 8, LANES), BF),
            pltpu.SemaphoreType.DMA((4,)),
        ],
        compiler_params=pltpu.CompilerParams(vmem_limit_bytes=8 * 2**20),
        cost_estimate=pl.CostEstimate(flops=10**6, bytes_accessed=3 * 10**6, transcendentals=0),
        name="core",
    )(keep, got, row)
    parts = lax.all_to_all(ready, FS_TP[:2], 0, 0, tiled=True)
    sums = pl.pallas_call(
        stop_kernel,
        out_shape=[shape(tall, 3 * LANES)] * 4,
        in_specs=[VMEM] * 4,
        out_specs=[VMEM] * 4,
        compiler_params=pltpu.CompilerParams(vmem_limit_bytes=8 * 2**20),
        cost_estimate=pl.CostEstimate(flops=10**6, bytes_accessed=2 * 10**6, transcendentals=0),
        name="stop",
    )(far, near, back, stay)
    moved = []
    for k, by in enumerate((2, 6, -6, -2)):
        moved.append(shifted(sums[k], by))
    sums = moved

    made, chunk = pl.pallas_call(
        functools.partial(owner_kernel, (n_x, n_core, width, hidden, block)),
        out_shape=[shape(block, rows), shape(hidden + 1, 3 * LANES)],
        in_specs=[VMEM] * 9,
        out_specs=[VMEM] * 2,
        scratch_shapes=[pltpu.VMEM((LANES, LANES), F32)],
        compiler_params=pltpu.CompilerParams(vmem_limit_bytes=12 * 2**20),
        cost_estimate=pl.CostEstimate(flops=10**8, bytes_accessed=2 * 10**6, transcendentals=0),
        name="owner",
    )(parts, tok_t, cot_t, inv, gain_rows, *sums)
    everything = lax.all_gather(chunk, "rep", axis=0, tiled=False)
    grad_gate, grad_up, grad_down, grad_gain, grad_input = pl.pallas_call(
        out_kernel,
        out_shape=[shape(hidden, width, dtype=F32)] * 3
        + [shape(1, block, dtype=F32), shape(block, rows)],
        in_specs=[VMEM] * 2,
        out_specs=[VMEM] * 5,
        compiler_params=pltpu.CompilerParams(vmem_limit_bytes=12 * 2**20),
        name="out",
    )(everything, made)
    return (grad_input.T, grad_gain.reshape(block), grad_gate, grad_up, grad_down)


def solution(mesh):
    torus = Mesh(
        mesh.devices.reshape(mesh.shape["rep"], mesh.shape["fs"], 4, 2),
        ("rep", "fs", "tp_0", "tp_1"),
    )
    placed = (P("rep", FS_TP), P("rep", FS_TP), P(), P(FS_TP, None), P(FS_TP, None), P(FS_TP, None))
    return jax.shard_map(
        body,
        mesh=torus,
        in_specs=placed,
        out_specs=(P("rep", FS_TP), P(FS_TP), P(FS_TP, None), P(FS_TP, None), P(FS_TP, None)),
        check_vma=False,
    )
```

```python
import functools

import jax
import jax.numpy as jnp
from jax import lax
from jax.experimental import pallas as pl
from jax.experimental.pallas import tpu as pltpu
from jax.sharding import Mesh
from jax.sharding import PartitionSpec as P


EPS = 1e-06
BF = jnp.bfloat16
F32 = jnp.float32
LANES = 128
VMEM = pl.BlockSpec(memory_space=pltpu.VMEM)
ANY = pl.BlockSpec(memory_space=pl.ANY)


def gain_columns(gain_ref, out_ref):
    for q in range(gain_ref.shape[0]):
        row = jnp.broadcast_to(gain_ref[q : q + 1, :], (LANES, LANES))
        out_ref[q * LANES : (q + 1) * LANES, :] = row.T


def split_in_two(v):
    high = v.astype(BF)
    return high, (v - high.astype(F32)).astype(BF)


def square_sum(ref, tokens):
    slabs, block, _ = ref.shape

    def step(s, acc):
        v = ref[s, :, 0:tokens].astype(F32)
        v = v * v
        parts = [v[8 * k : 8 * k + 8, :] for k in range(block // 8)]
        while len(parts) > 1:
            parts = [a + b for a, b in zip(parts[::2], parts[1::2])]
        return acc + parts[0]

    return lax.fori_loop(0, slabs, step, jnp.zeros((8, tokens), F32), unroll=4)


def ready_kernel(
    tokens, own_ref, gate_w_ref, up_w_ref, down_w_ref, gain_ref, pair_ref, down_ref, columns_ref, square_ref
):
    hidden, width = gate_w_ref.shape
    padded = down_ref.shape[0]
    low = padded - 16
    pair_ref[low:padded, :] = jnp.zeros((16, width), BF)
    pair_ref[padded + low : 2 * padded, :] = jnp.zeros((16, width), BF)
    down_ref[low:padded, :] = jnp.zeros((16, width), BF)
    pair_ref[0:hidden, :] = gate_w_ref[...]
    pair_ref[padded : padded + hidden, :] = up_w_ref[...]
    down_ref[0:hidden, :] = down_w_ref[...]
    gain_columns(gain_ref, columns_ref)
    square_ref[...] = square_sum(own_ref, tokens)


def main_kernel(
    sizes,
    own_ref,
    other_ref,
    pair_s,
    down_s,
    gain_s,
    square_ref,
    keep_ref,
    send_ref,
    row_ref,
    inv_ref,
    far_ref,
    near_ref,
    back_ref,
    stay_ref,
    normed_s,
    cot_s,
    delta_s,
    hidden_s,
    part_s,
    grad_s,
):
    n_rep, n_fs, n_x, n_core, tokens, _, padded, width, block = sizes
    core = lax.rem(lax.axis_index("node"), 2)
    z = lax.axis_index("rep")
    tall = grad_s.shape[1]
    total = square_ref[...] + square_sum(other_ref, tokens)
    mean = jnp.sum(total, axis=0, keepdims=True) / width
    inv = lax.rsqrt(mean + EPS)
    inv_ref[...] = jnp.broadcast_to(inv, (8, tokens))

    def normalise(first, carry):
        for ref, which in ((own_ref, core), (other_ref, 1 - core)):
            for second in range(4):
                y = 2 * (n_fs // 2 - 1 - first // 2) + lax.rem(1 - second // 2 + which, 2)
                x = 2 * (n_x // 2 - 1 - lax.rem(first, 2)) + lax.rem(1 - second % 2 + which, 2)
                at = pl.multiple_of(((y * n_x + x) * n_core + which) * block, block)
                s = second * 8 + first
                v = ref[s, :, 0:tokens].astype(F32) * inv
                g = gain_s[pl.ds(at, block), :]
                v = v * jnp.concatenate([g] * (tokens // LANES), axis=1)
                normed_s[pl.ds(at, block), :] = v.astype(BF)
                cot_s[pl.ds(at, block), :] = ref[s, :, tokens : 2 * tokens]
        return carry

    lax.fori_loop(0, 8, normalise, 0)

    both = jnp.dot(pair_s[...], normed_s[...], preferred_element_type=F32)
    d_hidden = 0.5 * jnp.dot(down_s[...], cot_s[...], preferred_element_type=F32)
    gate = both[0:padded, :]
    up = both[padded : 2 * padded, :]
    sig = jax.nn.sigmoid(gate)
    active = gate * sig
    hidden_s[...] = (active * up).astype(BF)
    d_gate = (d_hidden * up * sig * (1.0 + gate * (1.0 - sig))).astype(BF)
    d_up = (d_hidden * active).astype(BF)
    delta_s[0:padded, :] = d_gate
    delta_s[padded : 2 * padded, :] = d_up
    row = jnp.sum(d_gate.astype(F32) * gate + d_up.astype(F32) * up, axis=0, keepdims=True)
    row_ref[...] = jnp.broadcast_to(row, (8, tokens))
    high, low_part = split_in_two(row)
    send_ref[n_fs * n_x] = jnp.concatenate(
        [high, low_part, jnp.zeros((block - 2, tokens), BF)], axis=0
    )

    step = 256
    for b in range(width // step):
        cols = slice(b * step, (b + 1) * step)
        value = lax.dot_general(
            pair_s[:, cols], delta_s[...], (((0,), (0,)), ((), ())), preferred_element_type=F32
        ).astype(BF)
        for k in range(step // block):
            part_s[b * (step // block) + k] = value[k * block : (k + 1) * block, :]

    def share(s, carry):
        keep_ref[s] = part_s[n_core * s + core]
        send_ref[s] = part_s[n_core * s + 1 - core]
        return carry

    lax.fori_loop(0, n_fs * n_x, share, 0, unroll=4)

    side = 1 - 2 * core
    for b in range(width // step):
        rows = slice(b * step, (b + 1) * step)
        two = lax.dot_general(
            delta_s[...], normed_s[rows, :], (((1,), (1,)), ((), ())), preferred_element_type=F32
        )
        one = 0.5 * lax.dot_general(
            hidden_s[...], cot_s[rows, :], (((1,), (1,)), ((), ())), preferred_element_type=F32
        )
        for k in range(step // LANES):
            at = b * (step // LANES) + k
            lanes = slice(k * LANES, (k + 1) * LANES)
            grad_s[at, :, 0:LANES] = two[0:tall, lanes].astype(BF)
            grad_s[at, :, LANES : 2 * LANES] = two[padded : padded + tall, lanes].astype(BF)
            grad_s[at, :, 2 * LANES : 3 * LANES] = one[0:tall, lanes].astype(BF)

    for i in range(4):
        for ref, base in ((far_ref, 4), (near_ref, 3), (back_ref, 1), (stay_ref, 2)):
            ref[i] = grad_s[lax.rem(z + side * (base + 4 * i) + 2 * n_rep, n_rep)]


def core_kernel(block, keep_ref, got_ref, row_ref, out_ref, slab_s, sems):
    slabs = got_ref.shape[0] - 1
    groups = got_ref.shape[2] // LANES
    pieces = sems.shape[0]
    each = slabs // pieces
    other = got_ref[slabs, 0:8, :].astype(F32)
    row = row_ref[0:1, :] + other[0:1, :] + other[1:2, :]
    high, low_part = split_in_two(row)
    tail = [v[:, k * LANES : (k + 1) * LANES] for v in (high, low_part) for k in range(groups)]
    tail = jnp.concatenate(tail + [jnp.zeros((8 - 2 * groups, LANES), BF)], axis=0)

    def add(s, carry):
        v = (keep_ref[s].astype(F32) + got_ref[s].astype(F32)).astype(BF)
        for k in range(groups):
            slab_s[s, k * block : (k + 1) * block, :] = v[:, k * LANES : (k + 1) * LANES]
        slab_s[s, groups * block : groups * block + 8, :] = tail
        return carry

    copies = []
    for p in range(pieces):
        lax.fori_loop(p * each, (p + 1) * each, add, 0, unroll=4)
        here = pl.ds(p * each, each)
        copies.append(pltpu.make_async_copy(slab_s.at[here], out_ref.at[here], sems.at[p]))
        copies[-1].start()
    for copy in copies:
        copy.wait()


def stop_kernel(far_ref, near_ref, back_ref, stay_ref, *out_refs):
    for i, out_ref in enumerate(out_refs):
        v = stay_ref[i].astype(F32) + far_ref[i].astype(F32)
        v = v + near_ref[i].astype(F32) + back_ref[i].astype(F32)
        out_ref[...] = v.astype(BF)


def owner_kernel(
    sizes,
    part_ref,
    tok_ref,
    cot_ref,
    inv_ref,
    gain_ref,
    a_ref,
    b_ref,
    c_ref,
    d_ref,
    input_ref,
    chunk_ref,
    column_s,
):
    _, _, width, hidden, block = sizes
    sources, rows, _ = part_ref.shape
    tokens = tok_ref.shape[1]
    groups = tokens // LANES

    def add(s, acc):
        return acc + part_ref[s].astype(F32)

    total = lax.fori_loop(0, sources, add, jnp.zeros((rows, LANES), F32), unroll=4)
    summed = jnp.concatenate([total[k * block : (k + 1) * block, :] for k in range(groups)], axis=1)
    at = groups * block
    row = [total[at + k : at + k + 1, :] + total[at + groups + k : at + groups + k + 1, :] for k in range(groups)]
    row = jnp.concatenate(row, axis=1) / width
    me = lax.axis_index("node")
    per = LANES // block
    mine = gain_ref[pl.ds(lax.div(me, per), 1), :]
    column_s[...] = jnp.broadcast_to(mine, (LANES, LANES)).T
    g = column_s[pl.ds(pl.multiple_of(lax.rem(me, per) * block, block), block), :]
    inv = inv_ref[0:1, :]
    d_unit = summed * jnp.concatenate([g] * groups, axis=1)
    unit = tok_ref[...].astype(F32) * inv
    input_ref[...] = (cot_ref[...].astype(F32) + inv * (d_unit - unit * row)).astype(BF)

    along = jnp.sum(unit * summed, axis=1, keepdims=True)
    square = jnp.concatenate(
        [jnp.broadcast_to(along, (block, LANES)), jnp.zeros((LANES - block, LANES), F32)], axis=0
    )
    v = square.T[0:8, :]
    high, mid = split_in_two(v)
    low = v - high.astype(F32) - mid.astype(F32)
    extra = jnp.concatenate([high.astype(F32), mid.astype(F32), low], axis=1)[0:1, :]
    chunk = a_ref[...].astype(F32) + b_ref[...].astype(F32) + c_ref[...].astype(F32) + d_ref[...].astype(F32)
    which = lax.broadcasted_iota(jnp.int32, chunk.shape, 0)
    chunk = jnp.where(which == hidden, jnp.broadcast_to(extra, chunk.shape), chunk)
    chunk_ref[...] = chunk[0 : hidden + 1, :].astype(BF)


def out_kernel(all_ref, made_ref, gate_ref, up_ref, down_ref, gain_ref, input_ref):
    n, tall, _ = all_ref.shape
    hidden = tall - 1
    input_ref[...] = made_ref[...]
    total = jnp.zeros((1, 3 * LANES), F32)
    for b in range(n):
        lanes = slice(b * LANES, (b + 1) * LANES)
        v = all_ref[b].astype(F32)
        gate_ref[:, lanes] = v[0:hidden, 0:LANES]
        up_ref[:, lanes] = v[0:hidden, LANES : 2 * LANES]
        down_ref[:, lanes] = v[0:hidden, 2 * LANES : 3 * LANES]
        total = total + v[hidden : hidden + 1, :]
    gain = total[:, 0:LANES] + total[:, LANES : 2 * LANES] + total[:, 2 * LANES : 3 * LANES]
    gain_ref[...] = gain[:, 0 : gain_ref.shape[1]]


def spread(block, groups):
    copies = jnp.broadcast_to(block[None], (len(groups[0]),) + block.shape)
    return lax.all_to_all(copies, "node", 0, 0, tiled=True, axis_index_groups=groups)


def gather_groups(n_fs, n_x):
    def node(y, x, core):
        return (y % n_fs * n_x + x % n_x) * 2 + core

    cores, halves = range(2), range(2)
    wide = [
        [node(y, x, core) for y in range(n_fs - 2 + p, -1, -2) for x in range(n_x - 2 + q, -1, -2)]
        for core in cores
        for p in halves
        for q in halves
    ]
    near = [
        [node(2 * j + core + a, 2 * i + core + b, core) for a in (1, 0) for b in (1, 0)]
        for core in cores
        for j in range(n_fs // 2)
        for i in range(n_x // 2)
    ]
    return wide, near


def swapped(v):
    n = lax.axis_size("node")
    return lax.ppermute(v, "node", [(k, k ^ 1) for k in range(n)])


def shifted(v, by):
    n, m = lax.axis_size("rep"), lax.axis_size("node")
    pairs = []
    for z in range(n):
        for k in range(m):
            to = (z - by if k % 2 else z + by) % n
            pairs.append((z * m + k, to * m + k))
    return lax.ppermute(v, ("rep", "node"), pairs)


def body(tokens, cotangent, gain, w_gate, w_up, w_down):
    n_rep = lax.axis_size("rep")
    n_fs, n_x, n_core = 8, 4, 2
    wide, near = gather_groups(n_fs, n_x)
    peers = n_fs * n_x
    rows, block = tokens.shape
    width = gain.shape[0]
    hidden = w_gate.shape[0]
    padded = -(-hidden // 32) * 32
    tall = -(-hidden // 8) * 8
    n_blocks = width // LANES
    tok_t, cot_t = tokens.T, cotangent.T
    both = jnp.concatenate([tok_t, cot_t], axis=1)
    patch = spread(both, wide)
    plane = spread(patch.reshape(8 * block, 2 * rows), near)
    plane = plane.reshape(peers, block, 2 * rows)
    other = swapped(plane)
    gain_rows = gain.reshape(n_blocks, LANES)

    def shape(*dims, dtype=BF):
        return jax.ShapeDtypeStruct(dims, dtype)

    pair, down, columns, square = pl.pallas_call(
        functools.partial(ready_kernel, rows),
        out_shape=[
            shape(2 * padded, width),
            shape(padded, width),
            shape(width, LANES, dtype=F32),
            shape(8, rows, dtype=F32),
        ],
        in_specs=[VMEM] * 5,
        out_specs=[VMEM] * 4,
        compiler_params=pltpu.CompilerParams(vmem_limit_bytes=8 * 2**20),
        cost_estimate=pl.CostEstimate(flops=10**7, bytes_accessed=4 * 10**6, transcendentals=0),
        name="ready",
    )(plane, w_gate, w_up, w_down, gain_rows)

    sizes = (n_rep, n_fs, n_x, n_core, rows, hidden, padded, width, block)
    group = (4, tall, 3 * LANES)
    keep, send, row, inv, far, near, back, stay = pl.pallas_call(
        functools.partial(main_kernel, sizes),
        out_shape=[
            shape(peers, block, rows),
            shape(peers + 1, block, rows),
            shape(8, rows, dtype=F32),
            shape(8, rows, dtype=F32),
            shape(*group),
            shape(*group),
            shape(*group),
            shape(*group),
        ],
        in_specs=[VMEM] * 6,
        out_specs=[VMEM] * 8,
        scratch_shapes=[
            pltpu.VMEM((width, rows), BF),
            pltpu.VMEM((width, rows), BF),
            pltpu.VMEM((2 * padded, rows), BF),
            pltpu.VMEM((padded, rows), BF),
            pltpu.VMEM((peers * n_core, block, rows), BF),
            pltpu.VMEM((n_blocks, tall, 3 * LANES), BF),
        ],
        compiler_params=pltpu.CompilerParams(vmem_limit_bytes=34 * 2**20),
        cost_estimate=pl.CostEstimate(flops=11 * 10**8, bytes_accessed=10**7, transcendentals=0),
        name="main",
    )(plane, other, pair, down, columns, square)

    got = swapped(send)
    far = shifted(far, 2)
    near = shifted(near, 1)
    back = shifted(back, -1)
    ready = pl.pallas_call(
        functools.partial(core_kernel, block),
        out_shape=shape(peers, block * (rows // LANES) + 8, LANES),
        in_specs=[VMEM] * 3,
        out_specs=ANY,
        scratch_shapes=[
            pltpu.VMEM((peers, block * (rows // LANES) + 8, LANES), BF),
            pltpu.SemaphoreType.DMA((4,)),
        ],
        compiler_params=pltpu.CompilerParams(vmem_limit_bytes=8 * 2**20),
        cost_estimate=pl.CostEstimate(flops=10**6, bytes_accessed=3 * 10**6, transcendentals=0),
        name="core",
    )(keep, got, row)
    across = [[k * 2 + core for k in range(peers)] for core in range(2)]
    parts = lax.all_to_all(ready, "node", 0, 0, tiled=True, axis_index_groups=across)
    sums = pl.pallas_call(
        stop_kernel,
        out_shape=[shape(tall, 3 * LANES)] * 4,
        in_specs=[VMEM] * 4,
        out_specs=[VMEM] * 4,
        compiler_params=pltpu.CompilerParams(vmem_limit_bytes=8 * 2**20),
        cost_estimate=pl.CostEstimate(flops=10**6, bytes_accessed=2 * 10**6, transcendentals=0),
        name="stop",
    )(far, near, back, stay)
    moved = []
    for k, by in enumerate((2, 6, -6, -2)):
        moved.append(shifted(sums[k], by))
    sums = moved

    made, chunk = pl.pallas_call(
        functools.partial(owner_kernel, (n_x, n_core, width, hidden, block)),
        out_shape=[shape(block, rows), shape(hidden + 1, 3 * LANES)],
        in_specs=[VMEM] * 9,
        out_specs=[VMEM] * 2,
        scratch_shapes=[pltpu.VMEM((LANES, LANES), F32)],
        compiler_params=pltpu.CompilerParams(vmem_limit_bytes=12 * 2**20),
        cost_estimate=pl.CostEstimate(flops=10**8, bytes_accessed=2 * 10**6, transcendentals=0),
        name="owner",
    )(parts, tok_t, cot_t, inv, gain_rows, *sums)
    everything = lax.all_gather(chunk, "rep", axis=0, tiled=False)
    grad_gate, grad_up, grad_down, grad_gain, grad_input = pl.pallas_call(
        out_kernel,
        out_shape=[shape(hidden, width, dtype=F32)] * 3
        + [shape(1, block, dtype=F32), shape(block, rows)],
        in_specs=[VMEM] * 2,
        out_specs=[VMEM] * 5,
        compiler_params=pltpu.CompilerParams(vmem_limit_bytes=12 * 2**20),
        name="out",
    )(everything, made)
    return (grad_input.T, grad_gain.reshape(block), grad_gate, grad_up, grad_down)


def solution(mesh):
    torus = Mesh(
        mesh.devices.reshape(mesh.shape["rep"], 64),
        ("rep", "node"),
    )
    placed = (P("rep", "node"), P("rep", "node"), P(), P("node", None), P("node", None), P("node", None))
    return jax.shard_map(
        body,
        mesh=torus,
        in_specs=placed,
        out_specs=(P("rep", "node"), P("node"), P("node", None), P("node", None), P("node", None)),
        check_vma=False,
    )
```

```python
import functools

import jax
import jax.numpy as jnp
from jax import lax
from jax.experimental import pallas as pl
from jax.experimental.pallas import tpu as pltpu
from jax.sharding import Mesh
from jax.sharding import PartitionSpec as P


EPS = 1e-06
BF = jnp.bfloat16
F32 = jnp.float32
LANES = 128
FIRST = 12
VMEM = pl.BlockSpec(memory_space=pltpu.VMEM)
ANY = pl.BlockSpec(memory_space=pl.ANY)


def gain_columns(gain_ref, out_ref):
    for q in range(gain_ref.shape[0]):
        row = jnp.broadcast_to(gain_ref[q : q + 1, :], (LANES, LANES))
        out_ref[q * LANES : (q + 1) * LANES, :] = row.T


def split_in_two(v):
    high = v.astype(BF)
    return high, (v - high.astype(F32)).astype(BF)


def square_sum(ref, tokens):
    slabs, block, _ = ref.shape

    def step(s, acc):
        v = ref[s, :, 0:tokens].astype(F32)
        v = v * v
        parts = [v[8 * k : 8 * k + 8, :] for k in range(block // 8)]
        while len(parts) > 1:
            parts = [a + b for a, b in zip(parts[::2], parts[1::2])]
        return acc + parts[0]

    return lax.fori_loop(0, slabs, step, jnp.zeros((8, tokens), F32), unroll=4)


def ready_kernel(
    tokens, own_ref, gate_w_ref, up_w_ref, down_w_ref, gain_ref, pair_ref, down_ref, columns_ref, square_ref
):
    hidden, width = gate_w_ref.shape
    padded = down_ref.shape[0]
    low = padded - 16
    pair_ref[low:padded, :] = jnp.zeros((16, width), BF)
    pair_ref[padded + low : 2 * padded, :] = jnp.zeros((16, width), BF)
    down_ref[low:padded, :] = jnp.zeros((16, width), BF)
    pair_ref[0:hidden, :] = gate_w_ref[...]
    pair_ref[padded : padded + hidden, :] = up_w_ref[...]
    down_ref[0:hidden, :] = down_w_ref[...]
    gain_columns(gain_ref, columns_ref)
    square_ref[...] = square_sum(own_ref, tokens)


def main_kernel(
    sizes,
    own_ref,
    other_ref,
    pair_s,
    down_s,
    gain_s,
    square_ref,
    keep_ref,
    send_ref,
    row_ref,
    inv_ref,
    far_ref,
    near_ref,
    back_ref,
    stay_ref,
    normed_s,
    cot_s,
    delta_s,
    hidden_s,
    part_s,
    grad_s,
):
    n_rep, n_fs, n_x, n_core, tokens, _, padded, width, block = sizes
    core = lax.rem(lax.axis_index("node"), 2)
    z = lax.axis_index("rep")
    tall = grad_s.shape[1]
    total = square_ref[...] + square_sum(other_ref, tokens)
    mean = jnp.sum(total, axis=0, keepdims=True) / width
    inv = lax.rsqrt(mean + EPS)
    inv_ref[...] = jnp.broadcast_to(inv, (8, tokens))

    def normalise(first, carry):
        for ref, which in ((own_ref, core), (other_ref, 1 - core)):
            for second in range(4):
                y = 2 * lax.rem(n_fs // 2 - 1 - first // 2 + 3, n_fs // 2) + lax.rem(second // 2 + which, 2)
                x = 2 * (n_x // 2 - 1 - lax.rem(first, 2)) + lax.rem(1 - second % 2 + which, 2)
                at = pl.multiple_of(((y * n_x + x) * n_core + which) * block, block)
                s = second * 8 + first
                v = ref[s, :, 0:tokens].astype(F32) * inv
                g = gain_s[pl.ds(at, block), :]
                v = v * jnp.concatenate([g] * (tokens // LANES), axis=1)
                normed_s[pl.ds(at, block), :] = v.astype(BF)
                cot_s[pl.ds(at, block), :] = ref[s, :, tokens : 2 * tokens]
        return carry

    lax.fori_loop(0, 8, normalise, 0)

    both = jnp.dot(pair_s[...], normed_s[...], preferred_element_type=F32)
    d_hidden = 0.5 * jnp.dot(down_s[...], cot_s[...], preferred_element_type=F32)
    gate = both[0:padded, :]
    up = both[padded : 2 * padded, :]
    sig = jax.nn.sigmoid(gate)
    active = gate * sig
    hidden_s[...] = (active * up).astype(BF)
    d_gate = (d_hidden * up * sig * (1.0 + gate * (1.0 - sig))).astype(BF)
    d_up = (d_hidden * active).astype(BF)
    delta_s[0:padded, :] = d_gate
    delta_s[padded : 2 * padded, :] = d_up
    row = jnp.sum(d_gate.astype(F32) * gate + d_up.astype(F32) * up, axis=0, keepdims=True)
    row_ref[...] = jnp.broadcast_to(row, (8, tokens))
    high, low_part = split_in_two(row)
    send_ref[n_fs * n_x] = jnp.concatenate(
        [high, low_part, jnp.zeros((block - 2, tokens), BF)], axis=0
    )

    step = 256
    for b in range(width // step):
        cols = slice(b * step, (b + 1) * step)
        value = lax.dot_general(
            pair_s[:, cols], delta_s[...], (((0,), (0,)), ((), ())), preferred_element_type=F32
        ).astype(BF)
        for k in range(step // block):
            part_s[b * (step // block) + k] = value[k * block : (k + 1) * block, :]

    def share(s, carry):
        keep_ref[s] = part_s[n_core * s + core]
        send_ref[s] = part_s[n_core * s + 1 - core]
        return carry

    lax.fori_loop(0, n_fs * n_x, share, 0, unroll=4)

    side = 1 - 2 * core
    for b in range(width // step):
        rows = slice(b * step, (b + 1) * step)
        two = lax.dot_general(
            delta_s[...], normed_s[rows, :], (((1,), (1,)), ((), ())), preferred_element_type=F32
        )
        one = 0.5 * lax.dot_general(
            hidden_s[...], cot_s[rows, :], (((1,), (1,)), ((), ())), preferred_element_type=F32
        )
        for k in range(step // LANES):
            at = b * (step // LANES) + k
            lanes = slice(k * LANES, (k + 1) * LANES)
            grad_s[at, :, 0:LANES] = two[0:tall, lanes].astype(BF)
            grad_s[at, :, LANES : 2 * LANES] = two[padded : padded + tall, lanes].astype(BF)
            grad_s[at, :, 2 * LANES : 3 * LANES] = one[0:tall, lanes].astype(BF)

    for i in range(4):
        for ref, base in ((far_ref, 2), (near_ref, 1), (back_ref, -1), (stay_ref, 0)):
            ref[i] = grad_s[lax.rem(z + side * (base + 4 * i) + 2 * n_rep, n_rep)]


def core_kernel(block, keep_ref, got_ref, row_ref, out_ref, slab_s, sems):
    slabs = got_ref.shape[0] - 1
    groups = got_ref.shape[2] // LANES
    pieces = sems.shape[0]
    each = slabs // pieces
    other = got_ref[slabs, 0:8, :].astype(F32)
    row = row_ref[0:1, :] + other[0:1, :] + other[1:2, :]
    high, low_part = split_in_two(row)
    tail = [v[:, k * LANES : (k + 1) * LANES] for v in (high, low_part) for k in range(groups)]
    tail = jnp.concatenate(tail + [jnp.zeros((8 - 2 * groups, LANES), BF)], axis=0)

    def add(at, carry):
        s = lax.rem(at + FIRST, slabs)
        v = keep_ref[s] + got_ref[s]
        for k in range(groups):
            slab_s[at, k * block : (k + 1) * block, :] = v[:, k * LANES : (k + 1) * LANES]
        slab_s[at, groups * block : groups * block + 8, :] = tail
        return carry

    copies = []
    for p in range(pieces):
        lax.fori_loop(p * each, (p + 1) * each, add, 0, unroll=4)
        here = pl.ds(p * each, each)
        copies.append(pltpu.make_async_copy(slab_s.at[here], out_ref.at[here], sems.at[p]))
        copies[-1].start()
    for copy in copies:
        copy.wait()


def stop_kernel(far_ref, near_ref, back_ref, stay_ref, *out_refs):
    for i, out_ref in enumerate(out_refs):
        v = stay_ref[i].astype(F32) + far_ref[i].astype(F32)
        v = v + near_ref[i].astype(F32) + back_ref[i].astype(F32)
        out_ref[...] = v.astype(out_ref.dtype)


def owner_kernel(
    sizes,
    part_ref,
    tok_ref,
    cot_ref,
    inv_ref,
    gain_ref,
    a_ref,
    b_ref,
    c_ref,
    d_ref,
    input_ref,
    chunk_ref,
    column_s,
):
    _, _, width, hidden, block = sizes
    sources, rows, _ = part_ref.shape
    tokens = tok_ref.shape[1]
    groups = tokens // LANES

    def add(s, acc):
        return acc + part_ref[s].astype(F32)

    total = lax.fori_loop(0, sources, add, jnp.zeros((rows, LANES), F32), unroll=4)
    summed = jnp.concatenate([total[k * block : (k + 1) * block, :] for k in range(groups)], axis=1)
    at = groups * block
    row = [total[at + k : at + k + 1, :] + total[at + groups + k : at + groups + k + 1, :] for k in range(groups)]
    row = jnp.concatenate(row, axis=1) / width
    me = lax.axis_index("node")
    per = LANES // block
    mine = gain_ref[pl.ds(lax.div(me, per), 1), :]
    column_s[...] = jnp.broadcast_to(mine, (LANES, LANES)).T
    g = column_s[pl.ds(pl.multiple_of(lax.rem(me, per) * block, block), block), :]
    inv = inv_ref[0:1, :]
    d_unit = summed * jnp.concatenate([g] * groups, axis=1)
    unit = tok_ref[...].astype(F32) * inv
    input_ref[...] = (cot_ref[...].astype(F32) + inv * (d_unit - unit * row)).astype(BF)

    along = jnp.sum(unit * summed, axis=1, keepdims=True)
    square = jnp.concatenate(
        [jnp.broadcast_to(along, (block, LANES)), jnp.zeros((LANES - block, LANES), F32)], axis=0
    )
    v = square.T[0:8, :]
    high, mid = split_in_two(v)
    low = v - high.astype(F32) - mid.astype(F32)
    extra = jnp.concatenate([high.astype(F32), mid.astype(F32), low], axis=1)[0:1, :]
    chunk = a_ref[...].astype(F32) + b_ref[...].astype(F32) + c_ref[...].astype(F32) + d_ref[...].astype(F32)
    which = lax.broadcasted_iota(jnp.int32, chunk.shape, 0)
    chunk = jnp.where(which == hidden, jnp.broadcast_to(extra, chunk.shape), chunk)
    chunk_ref[...] = chunk[0 : hidden + 1, :].astype(BF)


def out_kernel(all_ref, made_ref, gate_ref, up_ref, down_ref, gain_ref, input_ref):
    n, tall, _ = all_ref.shape
    hidden = tall - 1
    input_ref[...] = made_ref[...]
    total = jnp.zeros((1, 3 * LANES), F32)
    for b in range(n):
        lanes = slice(b * LANES, (b + 1) * LANES)
        v = all_ref[b].astype(F32)
        gate_ref[:, lanes] = v[0:hidden, 0:LANES]
        up_ref[:, lanes] = v[0:hidden, LANES : 2 * LANES]
        down_ref[:, lanes] = v[0:hidden, 2 * LANES : 3 * LANES]
        total = total + v[hidden : hidden + 1, :]
    gain = total[:, 0:LANES] + total[:, LANES : 2 * LANES] + total[:, 2 * LANES : 3 * LANES]
    gain_ref[...] = gain[:, 0 : gain_ref.shape[1]]


def spread(block, groups):
    copies = jnp.broadcast_to(block[None], (len(groups[0]),) + block.shape)
    return lax.all_to_all(copies, "node", 0, 0, tiled=True, axis_index_groups=groups)


def gather_groups(n_fs, n_x):
    def node(y, x, core):
        return (y % n_fs * n_x + x % n_x) * 2 + core

    cores, halves = range(2), range(2)
    wide = [
        [node(y, x, core) for y in [(k + 6) % n_fs + p for k in range(n_fs - 2, -1, -2)] for x in range(n_x - 2 + q, -1, -2)]
        for core in cores
        for p in halves
        for q in halves
    ]
    near = [
        [node(2 * j + core + a, 2 * i + core + b, core) for a in (0, 1) for b in (1, 0)]
        for core in cores
        for j in range(n_fs // 2)
        for i in range(n_x // 2)
    ]
    return wide, near


def swapped(v):
    n = lax.axis_size("node")
    return lax.ppermute(v, "node", [(k, k ^ 1) for k in range(n)])


def shifted(v, by):
    n, m = lax.axis_size("rep"), lax.axis_size("node")
    pairs = []
    for z in range(n):
        for k in range(m):
            to = (z - by if k % 2 else z + by) % n
            pairs.append((z * m + k, to * m + k))
    return lax.ppermute(v, ("rep", "node"), pairs)


def body(tokens, cotangent, gain, w_gate, w_up, w_down):
    n_rep = lax.axis_size("rep")
    n_fs, n_x, n_core = 8, 4, 2
    wide, near = gather_groups(n_fs, n_x)
    peers = n_fs * n_x
    rows, block = tokens.shape
    width = gain.shape[0]
    hidden = w_gate.shape[0]
    padded = -(-hidden // 32) * 32
    tall = -(-hidden // 8) * 8
    n_blocks = width // LANES
    tok_t, cot_t = tokens.T, cotangent.T
    both = jnp.concatenate([tok_t, cot_t], axis=1)
    patch = spread(both, wide)
    plane = spread(patch.reshape(8 * block, 2 * rows), near)
    plane = plane.reshape(peers, block, 2 * rows)
    other = swapped(plane)
    gain_rows = gain.reshape(n_blocks, LANES)

    def shape(*dims, dtype=BF):
        return jax.ShapeDtypeStruct(dims, dtype)

    pair, down, columns, square = pl.pallas_call(
        functools.partial(ready_kernel, rows),
        out_shape=[
            shape(2 * padded, width),
            shape(padded, width),
            shape(width, LANES, dtype=F32),
            shape(8, rows, dtype=F32),
        ],
        in_specs=[VMEM] * 5,
        out_specs=[VMEM] * 4,
        compiler_params=pltpu.CompilerParams(vmem_limit_bytes=8 * 2**20),
        cost_estimate=pl.CostEstimate(flops=10**7, bytes_accessed=4 * 10**6, transcendentals=0),
        name="ready",
    )(plane, w_gate, w_up, w_down, gain_rows)

    sizes = (n_rep, n_fs, n_x, n_core, rows, hidden, padded, width, block)
    group = (4, tall, 3 * LANES)
    keep, send, row, inv, far, near, back, stay = pl.pallas_call(
        functools.partial(main_kernel, sizes),
        out_shape=[
            shape(peers, block, rows),
            shape(peers + 1, block, rows),
            shape(8, rows, dtype=F32),
            shape(8, rows, dtype=F32),
            shape(*group),
            shape(*group),
            shape(*group),
            shape(*group),
        ],
        in_specs=[VMEM] * 6,
        out_specs=[VMEM] * 8,
        scratch_shapes=[
            pltpu.VMEM((width, rows), BF),
            pltpu.VMEM((width, rows), BF),
            pltpu.VMEM((2 * padded, rows), BF),
            pltpu.VMEM((padded, rows), BF),
            pltpu.VMEM((peers * n_core, block, rows), BF),
            pltpu.VMEM((n_blocks, tall, 3 * LANES), BF),
        ],
        compiler_params=pltpu.CompilerParams(vmem_limit_bytes=34 * 2**20),
        cost_estimate=pl.CostEstimate(flops=11 * 10**8, bytes_accessed=10**7, transcendentals=0),
        name="main",
    )(plane, other, pair, down, columns, square)

    got = swapped(send)
    far = shifted(far, 2)
    near = shifted(near, 1)
    back = shifted(back, -1)
    ready = pl.pallas_call(
        functools.partial(core_kernel, block),
        out_shape=shape(peers, block * (rows // LANES) + 8, LANES),
        in_specs=[VMEM] * 3,
        out_specs=ANY,
        scratch_shapes=[
            pltpu.VMEM((peers, block * (rows // LANES) + 8, LANES), BF),
            pltpu.SemaphoreType.DMA((4,)),
        ],
        compiler_params=pltpu.CompilerParams(vmem_limit_bytes=8 * 2**20),
        cost_estimate=pl.CostEstimate(flops=10**6, bytes_accessed=3 * 10**6, transcendentals=0),
        name="core",
    )(keep, got, row)
    across = [[(k + FIRST) % peers * 2 + core for k in range(peers)] for core in range(2)]
    parts = lax.all_to_all(ready, "node", 0, 0, tiled=True, axis_index_groups=across)
    sums = pl.pallas_call(
        stop_kernel,
        out_shape=[shape(tall, 3 * LANES, dtype=F32)] + [shape(tall, 3 * LANES)] * 3,
        in_specs=[VMEM] * 4,
        out_specs=[VMEM] * 4,
        compiler_params=pltpu.CompilerParams(vmem_limit_bytes=8 * 2**20),
        cost_estimate=pl.CostEstimate(flops=10**6, bytes_accessed=2 * 10**6, transcendentals=0),
        name="stop",
    )(far, near, back, stay)
    moved = [sums[0]]
    for k, by in ((1, 4), (2, 8), (3, -4)):
        moved.append(shifted(sums[k], by))
    sums = moved

    made, chunk = pl.pallas_call(
        functools.partial(owner_kernel, (n_x, n_core, width, hidden, block)),
        out_shape=[shape(block, rows), shape(hidden + 1, 3 * LANES)],
        in_specs=[VMEM] * 9,
        out_specs=[VMEM] * 2,
        scratch_shapes=[pltpu.VMEM((LANES, LANES), F32)],
        compiler_params=pltpu.CompilerParams(vmem_limit_bytes=12 * 2**20),
        cost_estimate=pl.CostEstimate(flops=10**8, bytes_accessed=2 * 10**6, transcendentals=0),
        name="owner",
    )(parts, tok_t, cot_t, inv, gain_rows, *sums)
    everything = lax.all_gather(chunk, "rep", axis=0, tiled=False)
    grad_gate, grad_up, grad_down, grad_gain, grad_input = pl.pallas_call(
        out_kernel,
        out_shape=[shape(hidden, width, dtype=F32)] * 3
        + [shape(1, block, dtype=F32), shape(block, rows)],
        in_specs=[VMEM] * 2,
        out_specs=[VMEM] * 5,
        compiler_params=pltpu.CompilerParams(vmem_limit_bytes=12 * 2**20),
        name="out",
    )(everything, made)
    return (grad_input.T, grad_gain.reshape(block), grad_gate, grad_up, grad_down)


def solution(mesh):
    torus = Mesh(
        mesh.devices.reshape(mesh.shape["rep"], 64),
        ("rep", "node"),
    )
    placed = (P("rep", "node"), P("rep", "node"), P(), P("node", None), P("node", None), P("node", None))
    return jax.shard_map(
        body,
        mesh=torus,
        in_specs=placed,
        out_specs=(P("rep", "node"), P("node"), P("node", None), P("node", None), P("node", None)),
        check_vma=False,
    )
```

```python
import functools

import jax
import jax.numpy as jnp
from jax import lax
from jax.experimental import pallas as pl
from jax.experimental.pallas import tpu as pltpu
from jax.sharding import Mesh
from jax.sharding import PartitionSpec as P


EPS = 1e-06
BF = jnp.bfloat16
F32 = jnp.float32
LANES = 128
FIRST = 12
VMEM = pl.BlockSpec(memory_space=pltpu.VMEM)
ANY = pl.BlockSpec(memory_space=pl.ANY)


def gain_columns(gain_ref, out_ref):
    for q in range(gain_ref.shape[0]):
        row = jnp.broadcast_to(gain_ref[q : q + 1, :], (LANES, LANES))
        out_ref[q * LANES : (q + 1) * LANES, :] = row.T


def split_in_two(v):
    high = v.astype(BF)
    return high, (v - high.astype(F32)).astype(BF)


def square_sum(ref, tokens):
    slabs, block, _ = ref.shape

    def step(s, acc):
        v = ref[s, :, 0:tokens].astype(F32)
        v = v * v
        parts = [v[8 * k : 8 * k + 8, :] for k in range(block // 8)]
        while len(parts) > 1:
            parts = [a + b for a, b in zip(parts[::2], parts[1::2])]
        return acc + parts[0]

    return lax.fori_loop(0, slabs, step, jnp.zeros((8, tokens), F32), unroll=4)


def ready_kernel(
    tokens, own_ref, gate_w_ref, up_w_ref, down_w_ref, gain_ref, pair_ref, down_ref, columns_ref, square_ref
):
    hidden, width = gate_w_ref.shape
    padded = down_ref.shape[0]
    low = padded - 16
    pair_ref[low:padded, :] = jnp.zeros((16, width), BF)
    pair_ref[padded + low : 2 * padded, :] = jnp.zeros((16, width), BF)
    down_ref[low:padded, :] = jnp.zeros((16, width), BF)
    pair_ref[0:hidden, :] = gate_w_ref[...]
    pair_ref[padded : padded + hidden, :] = up_w_ref[...]
    down_ref[0:hidden, :] = down_w_ref[...]
    gain_columns(gain_ref, columns_ref)
    square_ref[...] = square_sum(own_ref, tokens)


def main_kernel(
    sizes,
    own_ref,
    other_ref,
    pair_s,
    down_s,
    gain_s,
    square_ref,
    keep_ref,
    send_ref,
    row_ref,
    inv_ref,
    far_ref,
    near_ref,
    back_ref,
    stay_ref,
    normed_s,
    cot_s,
    delta_s,
    hidden_s,
    part_s,
    grad_s,
):
    n_rep, n_fs, n_x, n_core, tokens, _, padded, width, block = sizes
    core = lax.rem(lax.axis_index("node"), 2)
    z = lax.axis_index("rep")
    tall = grad_s.shape[1]
    total = square_ref[...] + square_sum(other_ref, tokens)
    mean = jnp.sum(total, axis=0, keepdims=True) / width
    inv = lax.rsqrt(mean + EPS)
    inv_ref[...] = jnp.broadcast_to(inv, (8, tokens))

    def normalise(first, carry):
        for ref, which in ((own_ref, core), (other_ref, 1 - core)):
            for second in range(4):
                y = 2 * lax.rem(n_fs // 2 - 1 - first // 2 + 3, n_fs // 2) + lax.rem(second // 2 + which, 2)
                x = 2 * (n_x // 2 - 1 - lax.rem(first, 2)) + lax.rem(1 - second % 2 + which, 2)
                at = pl.multiple_of(((y * n_x + x) * n_core + which) * block, block)
                s = second * 8 + first
                v = ref[s, :, 0:tokens].astype(F32) * inv
                g = gain_s[pl.ds(at, block), :]
                v = v * jnp.concatenate([g] * (tokens // LANES), axis=1)
                normed_s[pl.ds(at, block), :] = v.astype(BF)
                cot_s[pl.ds(at, block), :] = ref[s, :, tokens : 2 * tokens]
        return carry

    lax.fori_loop(0, 8, normalise, 0)

    both = jnp.dot(pair_s[...], normed_s[...], preferred_element_type=F32)
    d_hidden = 0.5 * jnp.dot(down_s[...], cot_s[...], preferred_element_type=F32)
    gate = both[0:padded, :]
    up = both[padded : 2 * padded, :]
    sig = jax.nn.sigmoid(gate)
    active = gate * sig
    hidden_s[...] = (active * up).astype(BF)
    d_gate = (d_hidden * up * sig * (1.0 + gate * (1.0 - sig))).astype(BF)
    d_up = (d_hidden * active).astype(BF)
    delta_s[0:padded, :] = d_gate
    delta_s[padded : 2 * padded, :] = d_up
    row = jnp.sum(d_gate.astype(F32) * gate + d_up.astype(F32) * up, axis=0, keepdims=True)
    row_ref[...] = jnp.broadcast_to(row, (8, tokens))
    high, low_part = split_in_two(row)
    send_ref[n_fs * n_x] = jnp.concatenate(
        [high, low_part, jnp.zeros((block - 2, tokens), BF)], axis=0
    )

    step = 256
    for b in range(width // step):
        cols = slice(b * step, (b + 1) * step)
        value = lax.dot_general(
            pair_s[:, cols], delta_s[...], (((0,), (0,)), ((), ())), preferred_element_type=F32
        ).astype(BF)
        for k in range(step // block):
            part_s[b * (step // block) + k] = value[k * block : (k + 1) * block, :]

    def share(s, carry):
        keep_ref[s] = part_s[n_core * s + core]
        send_ref[s] = part_s[n_core * s + 1 - core]
        return carry

    lax.fori_loop(0, n_fs * n_x, share, 0, unroll=4)

    side = 2 * core - 1
    for b in range(width // step):
        rows = slice(b * step, (b + 1) * step)
        two = lax.dot_general(
            delta_s[...], normed_s[rows, :], (((1,), (1,)), ((), ())), preferred_element_type=F32
        )
        one = 0.5 * lax.dot_general(
            hidden_s[...], cot_s[rows, :], (((1,), (1,)), ((), ())), preferred_element_type=F32
        )
        for k in range(step // LANES):
            at = b * (step // LANES) + k
            lanes = slice(k * LANES, (k + 1) * LANES)
            grad_s[at, :, 0:LANES] = two[0:tall, lanes].astype(BF)
            grad_s[at, :, LANES : 2 * LANES] = two[padded : padded + tall, lanes].astype(BF)
            grad_s[at, :, 2 * LANES : 3 * LANES] = one[0:tall, lanes].astype(BF)

    for i in range(4):
        for ref, base in ((far_ref, 2), (near_ref, 1), (back_ref, -1), (stay_ref, 0)):
            ref[i] = grad_s[lax.rem(z + side * (base + 4 * i) + 2 * n_rep, n_rep)]


def core_kernel(block, keep_ref, got_ref, row_ref, out_ref, slab_s, sems):
    slabs = got_ref.shape[0] - 1
    groups = got_ref.shape[2] // LANES
    pieces = sems.shape[0]
    each = slabs // pieces
    other = got_ref[slabs, 0:8, :].astype(F32)
    row = row_ref[0:1, :] + other[0:1, :] + other[1:2, :]
    high, low_part = split_in_two(row)
    tail = [v[:, k * LANES : (k + 1) * LANES] for v in (high, low_part) for k in range(groups)]
    tail = jnp.concatenate(tail + [jnp.zeros((8 - 2 * groups, LANES), BF)], axis=0)

    def add(at, carry):
        s = lax.rem(at + FIRST, slabs)
        v = keep_ref[s] + got_ref[s]
        for k in range(groups):
            slab_s[at, k * block : (k + 1) * block, :] = v[:, k * LANES : (k + 1) * LANES]
        slab_s[at, groups * block : groups * block + 8, :] = tail
        return carry

    copies = []
    for p in range(pieces):
        lax.fori_loop(p * each, (p + 1) * each, add, 0, unroll=4)
        here = pl.ds(p * each, each)
        copies.append(pltpu.make_async_copy(slab_s.at[here], out_ref.at[here], sems.at[p]))
        copies[-1].start()
    for copy in copies:
        copy.wait()


def stop_kernel(far_ref, near_ref, back_ref, stay_ref, *out_refs):
    for i, out_ref in enumerate(out_refs):
        v = stay_ref[i].astype(F32) + far_ref[i].astype(F32)
        v = v + near_ref[i].astype(F32) + back_ref[i].astype(F32)
        out_ref[...] = v.astype(out_ref.dtype)


def owner_kernel(
    sizes,
    part_ref,
    tok_ref,
    cot_ref,
    inv_ref,
    gain_ref,
    a_ref,
    b_ref,
    c_ref,
    d_ref,
    input_ref,
    chunk_ref,
    column_s,
):
    _, _, width, hidden, block = sizes
    sources, rows, _ = part_ref.shape
    tokens = tok_ref.shape[1]
    groups = tokens // LANES

    def add(s, acc):
        return acc + part_ref[s].astype(F32)

    total = lax.fori_loop(0, sources, add, jnp.zeros((rows, LANES), F32), unroll=4)
    summed = jnp.concatenate([total[k * block : (k + 1) * block, :] for k in range(groups)], axis=1)
    at = groups * block
    row = [total[at + k : at + k + 1, :] + total[at + groups + k : at + groups + k + 1, :] for k in range(groups)]
    row = jnp.concatenate(row, axis=1) / width
    me = lax.axis_index("node")
    per = LANES // block
    mine = gain_ref[pl.ds(lax.div(me, per), 1), :]
    column_s[...] = jnp.broadcast_to(mine, (LANES, LANES)).T
    g = column_s[pl.ds(pl.multiple_of(lax.rem(me, per) * block, block), block), :]
    inv = inv_ref[0:1, :]
    d_unit = summed * jnp.concatenate([g] * groups, axis=1)
    unit = tok_ref[...].astype(F32) * inv
    input_ref[...] = (cot_ref[...].astype(F32) + inv * (d_unit - unit * row)).astype(BF)

    along = jnp.sum(unit * summed, axis=1, keepdims=True)
    square = jnp.concatenate(
        [jnp.broadcast_to(along, (block, LANES)), jnp.zeros((LANES - block, LANES), F32)], axis=0
    )
    v = square.T[0:8, :]
    high, mid = split_in_two(v)
    low = v - high.astype(F32) - mid.astype(F32)
    extra = jnp.concatenate([high.astype(F32), mid.astype(F32), low], axis=1)[0:1, :]
    chunk = a_ref[...].astype(F32) + b_ref[...].astype(F32) + c_ref[...].astype(F32) + d_ref[...].astype(F32)
    which = lax.broadcasted_iota(jnp.int32, chunk.shape, 0)
    chunk = jnp.where(which == hidden, jnp.broadcast_to(extra, chunk.shape), chunk)
    chunk_ref[...] = chunk[0 : hidden + 1, :].astype(BF)


def out_kernel(all_ref, made_ref, gate_ref, up_ref, down_ref, gain_ref, input_ref):
    n, tall, _ = all_ref.shape
    hidden = tall - 1
    input_ref[...] = made_ref[...]
    total = jnp.zeros((1, 3 * LANES), F32)
    for b in range(n):
        lanes = slice(b * LANES, (b + 1) * LANES)
        v = all_ref[b].astype(F32)
        gate_ref[:, lanes] = v[0:hidden, 0:LANES]
        up_ref[:, lanes] = v[0:hidden, LANES : 2 * LANES]
        down_ref[:, lanes] = v[0:hidden, 2 * LANES : 3 * LANES]
        total = total + v[hidden : hidden + 1, :]
    gain = total[:, 0:LANES] + total[:, LANES : 2 * LANES] + total[:, 2 * LANES : 3 * LANES]
    gain_ref[...] = gain[:, 0 : gain_ref.shape[1]]


def spread(block, groups):
    copies = jnp.broadcast_to(block[None], (len(groups[0]),) + block.shape)
    return lax.all_to_all(copies, "node", 0, 0, tiled=True, axis_index_groups=groups)


def gather_groups(n_fs, n_x):
    def node(y, x, core):
        return (y % n_fs * n_x + x % n_x) * 2 + core

    cores, halves = range(2), range(2)
    wide = [
        [node(y, x, core) for y in [(k + 6) % n_fs + p for k in range(n_fs - 2, -1, -2)] for x in range(n_x - 2 + q, -1, -2)]
        for core in cores
        for p in halves
        for q in halves
    ]
    near = [
        [node(2 * j + core + a, 2 * i + core + b, core) for a in (0, 1) for b in (1, 0)]
        for core in cores
        for j in range(n_fs // 2)
        for i in range(n_x // 2)
    ]
    return wide, near


def swapped(v):
    n = lax.axis_size("node")
    return lax.ppermute(v, "node", [(k, k ^ 1) for k in range(n)])


def shifted(v, by):
    n, m = lax.axis_size("rep"), lax.axis_size("node")
    pairs = []
    for z in range(n):
        for k in range(m):
            to = (z + by if k % 2 else z - by) % n
            pairs.append((z * m + k, to * m + k))
    return lax.ppermute(v, ("rep", "node"), pairs)


def body(tokens, cotangent, gain, w_gate, w_up, w_down):
    n_rep = lax.axis_size("rep")
    n_fs, n_x, n_core = 8, 4, 2
    wide, near = gather_groups(n_fs, n_x)
    peers = n_fs * n_x
    rows, block = tokens.shape
    width = gain.shape[0]
    hidden = w_gate.shape[0]
    padded = -(-hidden // 32) * 32
    tall = -(-hidden // 8) * 8
    n_blocks = width // LANES
    tok_t, cot_t = tokens.T, cotangent.T
    both = jnp.concatenate([tok_t, cot_t], axis=1)
    patch = spread(both, wide)
    plane = spread(patch.reshape(8 * block, 2 * rows), near)
    plane = plane.reshape(peers, block, 2 * rows)
    other = swapped(plane)
    gain_rows = gain.reshape(n_blocks, LANES)

    def shape(*dims, dtype=BF):
        return jax.ShapeDtypeStruct(dims, dtype)

    pair, down, columns, square = pl.pallas_call(
        functools.partial(ready_kernel, rows),
        out_shape=[
            shape(2 * padded, width),
            shape(padded, width),
            shape(width, LANES, dtype=F32),
            shape(8, rows, dtype=F32),
        ],
        in_specs=[VMEM] * 5,
        out_specs=[VMEM] * 4,
        compiler_params=pltpu.CompilerParams(vmem_limit_bytes=8 * 2**20),
        cost_estimate=pl.CostEstimate(flops=10**7, bytes_accessed=4 * 10**6, transcendentals=0),
        name="ready",
    )(plane, w_gate, w_up, w_down, gain_rows)

    sizes = (n_rep, n_fs, n_x, n_core, rows, hidden, padded, width, block)
    group = (4, tall, 3 * LANES)
    keep, send, row, inv, far, near, back, stay = pl.pallas_call(
        functools.partial(main_kernel, sizes),
        out_shape=[
            shape(peers, block, rows),
            shape(peers + 1, block, rows),
            shape(8, rows, dtype=F32),
            shape(8, rows, dtype=F32),
            shape(*group),
            shape(*group),
            shape(*group),
            shape(*group),
        ],
        in_specs=[VMEM] * 6,
        out_specs=[VMEM] * 8,
        scratch_shapes=[
            pltpu.VMEM((width, rows), BF),
            pltpu.VMEM((width, rows), BF),
            pltpu.VMEM((2 * padded, rows), BF),
            pltpu.VMEM((padded, rows), BF),
            pltpu.VMEM((peers * n_core, block, rows), BF),
            pltpu.VMEM((n_blocks, tall, 3 * LANES), BF),
        ],
        compiler_params=pltpu.CompilerParams(vmem_limit_bytes=34 * 2**20),
        cost_estimate=pl.CostEstimate(flops=11 * 10**8, bytes_accessed=10**7, transcendentals=0),
        name="main",
    )(plane, other, pair, down, columns, square)

    got = swapped(send)
    far = shifted(far, 2)
    near = shifted(near, 1)
    back = shifted(back, -1)
    ready = pl.pallas_call(
        functools.partial(core_kernel, block),
        out_shape=shape(peers, block * (rows // LANES) + 8, LANES),
        in_specs=[VMEM] * 3,
        out_specs=ANY,
        scratch_shapes=[
            pltpu.VMEM((peers, block * (rows // LANES) + 8, LANES), BF),
            pltpu.SemaphoreType.DMA((8,)),
        ],
        compiler_params=pltpu.CompilerParams(vmem_limit_bytes=8 * 2**20),
        cost_estimate=pl.CostEstimate(flops=10**6, bytes_accessed=3 * 10**6, transcendentals=0),
        name="core",
    )(keep, got, row)
    across = [[(k + FIRST) % peers * 2 + core for k in range(peers)] for core in range(2)]
    parts = lax.all_to_all(ready, "node", 0, 0, tiled=True, axis_index_groups=across)
    sums = pl.pallas_call(
        stop_kernel,
        out_shape=[shape(tall, 3 * LANES, dtype=F32)] + [shape(tall, 3 * LANES)] * 3,
        in_specs=[VMEM] * 4,
        out_specs=[VMEM] * 4,
        compiler_params=pltpu.CompilerParams(vmem_limit_bytes=8 * 2**20),
        cost_estimate=pl.CostEstimate(flops=10**6, bytes_accessed=2 * 10**6, transcendentals=0),
        name="stop",
    )(far, near, back, stay)
    moved = [sums[0]]
    for k, by in ((1, 4), (2, 8), (3, -4)):
        moved.append(shifted(sums[k], by))
    sums = moved

    made, chunk = pl.pallas_call(
        functools.partial(owner_kernel, (n_x, n_core, width, hidden, block)),
        out_shape=[shape(block, rows), shape(hidden + 1, 3 * LANES)],
        in_specs=[VMEM] * 9,
        out_specs=[VMEM] * 2,
        scratch_shapes=[pltpu.VMEM((LANES, LANES), F32)],
        compiler_params=pltpu.CompilerParams(vmem_limit_bytes=12 * 2**20),
        cost_estimate=pl.CostEstimate(flops=10**8, bytes_accessed=2 * 10**6, transcendentals=0),
        name="owner",
    )(parts, tok_t, cot_t, inv, gain_rows, *sums)
    everything = lax.all_gather(chunk, "rep", axis=0, tiled=False)
    grad_gate, grad_up, grad_down, grad_gain, grad_input = pl.pallas_call(
        out_kernel,
        out_shape=[shape(hidden, width, dtype=F32)] * 3
        + [shape(1, block, dtype=F32), shape(block, rows)],
        in_specs=[VMEM] * 2,
        out_specs=[VMEM] * 5,
        compiler_params=pltpu.CompilerParams(vmem_limit_bytes=12 * 2**20),
        name="out",
    )(everything, made)
    return (grad_input.T, grad_gain.reshape(block), grad_gate, grad_up, grad_down)


def solution(mesh):
    torus = Mesh(
        mesh.devices.reshape(mesh.shape["rep"], 64),
        ("rep", "node"),
    )
    placed = (P("rep", "node"), P("rep", "node"), P(), P("node", None), P("node", None), P("node", None))
    return jax.shard_map(
        body,
        mesh=torus,
        in_specs=placed,
        out_specs=(P("rep", "node"), P("node"), P("node", None), P("node", None), P("node", None)),
        check_vma=False,
    )
```
